256 devices in a mesh: sp: 64 (over z, x, core), tp: 4 (over y).
Axes of the slice: x: 4, y: 4, z: 8, core: 2. Of those that a mesh axis runs over, the one named last changes fastest.
Arguments:
- cot_out: bfloat16 [16384, 2048], P('sp', 'tp'), may hold values from -16 to 16
- route_ids: int32 [16384, 2], P('sp'), may hold values from 0 to 63, all different within a row; in each aligned block of 256 rows (0 to 255, 256 to 511, ...) at most 12 rows name the same one
- route_weight: float32 [16384, 2], P('sp'), may hold values from 0.1 to 1
- expert_inputs: bfloat16 [64, 768, 2048], P('sp'), may hold values from -48 to 48
- w_gate: bfloat16 [64, 2048, 1024], P('sp', None, 'tp'), may hold values from -0.125 to 0.125
- w_up: bfloat16 [64, 2048, 1024], P('sp', None, 'tp'), may hold values from -0.125 to 0.125
- w_down: bfloat16 [64, 1024, 2048], P('sp', 'tp'), may hold values from -0.1875 to 0.1875
- w_proj: bfloat16 [2048, 2048], P('tp'), may hold values from -0.125 to 0.125
- conv_out: bfloat16 [16384, 2048], P('sp', 'tp'), may hold values from -6 to 6
- channel_norm_gain: float32 [2048], P('tp'), may hold values from 0.1 to 1.9
- taps: float32 [31, 2048], P(None, 'tp'), may hold values from -1 to 1
- value_pre: bfloat16 [16384, 2048], P('sp', 'tp'), may hold values from -6 to 6
- gate_pre: bfloat16 [16384, 2048], P('sp', 'tp'), may hold values from -6 to 6
Outputs:
- grad_gate_w: bfloat16 [64, 2048, 1024], P('sp', None, 'tp')
- grad_up_w: bfloat16 [64, 2048, 1024], P('sp', None, 'tp')
- grad_down_w: bfloat16 [64, 1024, 2048], P('sp', 'tp')
- grad_proj: float32 [2048, 2048], P(('tp', 'sp'))
- grad_value: bfloat16 [16384, 2048], P('sp', 'tp')
- grad_gate: bfloat16 [16384, 2048], P('sp', 'tp')
The draws below stay inside these ranges and needn't reach their ends.
Inputs may be any that keep to these rules, and one draw needn't show every extreme that they name: `route_ids`: among the tokens of one index of sp no expert is chosen more than 12 times, a bound that some block reaches; a token's experts differ.
All inputs are finite; a program needn't handle non-finite values.
Results may differ from the reference program's by a relative error of at most 0.012.
Values may be sent and summed in bfloat16 or wider, within the bound.
No kernel may reach another device: no remote copies, remote signals or barrier semaphores. Data moves between devices by JAX's collectives and lax.ppermute only.
A program may use at most 128 MiB of HBM per device.

```python
import math
import jax
import jax.numpy as jnp
import numpy as np
from jax import lax

D = 2048
F = 1024
WIDTH = 31
TOP = 2
TOK_DEV = 256
EXPERTS = 64
CAP = 12
SLOTS = 768
TOKENS = 16384
N_SP = 64
N_TP = 4


def draw_expert_inputs(key, part):
    keys = jax.random.split(jax.random.fold_in(key, 11), 2)
    shape = (EXPERTS, SLOTS, D)
    base = jax.random.truncated_normal(keys[0], -6.0, 6.0, shape, jnp.float32)
    scales = jnp.exp(jax.random.uniform(keys[1], (EXPERTS, SLOTS, 1), jnp.float32, jnp.log(0.5), jnp.log(6.0)))
    values = scales * base
    return jnp.clip(values, -48.0, 48.0).astype(jnp.bfloat16)


def spiked(values, own_key, source, target, parts, factor):
    def block_of(position):
        return (jnp.arange(values.shape[position]) // (values.shape[position] // parts)).reshape((-1,) + (1,) * (values.ndim - 1 - position))

    near = jax.random.permutation(own_key, parts)[block_of(target)]
    second = (block_of(target) + parts // 2) % parts
    return jnp.where((block_of(source) == near) | (block_of(source) == second), factor * values, values)


def level_of(own_key, dims, pieces, least, top_value):
    def one(axis_at, blocks):
        draws = jax.random.uniform(jax.random.fold_in(jax.random.fold_in(own_key, 6), axis_at), (blocks,), jnp.float32, least / len(pieces), top_value / len(pieces))
        return jnp.repeat(jnp.exp(draws), dims[axis_at] // blocks).reshape((-1,) + (1,) * (len(dims) - axis_at - 1))

    gain = one(*pieces[0])
    for cut in pieces[1:]:
        gain = gain * one(*cut)
    return gain


def shared_out(stream_key, own, number, rows, count, top, reach, lean):
    ranking = jax.random.permutation(stream_key, count)
    heavy_load, usual = shares(count, rows * top, reach, lean, True), shares(count, rows * top, reach, lean, False)
    places = jnp.arange(count)

    def named(tallies, offset_by):
        used = int((tallies > 0).sum())
        fixed = max(1, used // 4)
        passed = fixed + (places - fixed + offset_by * (used - fixed)) % max(1, count - fixed)
        return jnp.zeros((count,), jnp.int32).at[ranking[jnp.where(places < fixed, places, passed)]].set(jnp.asarray(tallies, jnp.int32))

    tallies = jnp.where(number % 4 == 0, named(heavy_load, number // 4), named(usual, number - number // 4 - 1))
    mixed = jax.random.permutation(jax.random.fold_in(own, 3), count)
    source_of, sink = mixed[0:count // 2 * 2:2], mixed[1:count // 2 * 2:2]
    room = jnp.minimum(tallies[source_of] - 1, reach - tallies[sink]) // 2
    room = jnp.where((source_of == ranking[0]) | (sink == ranking[0]) | (tallies[sink] == 0), 0, jnp.maximum(room, 0))
    passed = jax.random.randint(jax.random.fold_in(own, 4), (count // 2,), 0, 1 << 20) % (room + 1)
    tallies = tallies.at[source_of].add(-passed).at[sink].add(passed)
    members = jnp.searchsorted(jnp.cumsum(tallies), jnp.arange(rows * top), side="right").astype(jnp.int32)
    table = members.reshape(top, rows).T
    table = table[jax.random.permutation(jax.random.fold_in(own, 1), rows)]
    offset_by = jax.random.randint(jax.random.fold_in(own, 2), (rows, 1), 0, top)
    return jnp.take_along_axis(table, (jnp.arange(top)[None, :] + offset_by) % top, axis=1)


def shares(amount, total, limit, lean, full):
    portions = [(1 << 20) // math.isqrt(grade ** lean) + 1 for grade in range(1, amount + 1)]
    largest = limit if full else min(limit, max(-(-total // amount), total * portions[0] // sum(portions)))
    least = 1 if total - largest >= amount - 1 else 0
    given, rest = [largest] + [least] * (amount - 1), total - largest - least * (amount - 1)
    while rest > 0:
        free = [i for i in range(1, amount) if given[i] < largest] or [i for i in range(1, amount) if given[i] < limit]
        whole, budget = sum([portions[i] for i in free]), rest
        for i in free:
            extra = min(limit - given[i], max(1, budget * portions[i] // whole), rest)
            given[i] = given[i] + extra
            rest = rest - extra
    return np.array(given)


def centred(key, dims, width, most, cuts=(), held_as=jnp.bfloat16):
    drawn = jax.random.normal(key, dims, jnp.float32) * width
    if len(cuts) > 0:
        drawn = level_of(key, dims, cuts, -0.22, 0.18) * drawn
    return jnp.clip(drawn, min=-most, max=most).astype(held_as)


def gaussian_with(key, shape, spread, reach, shards, heavy, held_as=jnp.bfloat16):
    drawn = spread * jax.random.normal(key, shape, jnp.float32)
    if shards:
        drawn = drawn * level_of(key, shape, shards, -0.22, 0.18)
    return jnp.clip(spiked(drawn, jax.random.fold_in(key, 3), *heavy), -reach, reach).astype(held_as)


def setup_inputs(seed: int = 0) -> dict:
    seeds = jax.random.split(jax.random.key(seed), 14)
    cot_out = gaussian_with(seeds[0], (TOKENS, D), 1.0, 16.0, ((0, 64), (1, 4)), (0, 1, 64, 4.0))
    route_ids_keys = jax.random.split(jax.random.fold_in(seeds[1], 1), TOKENS // TOK_DEV)
    route_ids_turns = jax.random.permutation(jax.random.fold_in(seeds[1], 3), TOKENS // TOK_DEV)
    route_ids = jax.vmap(lambda own, number: shared_out(jax.random.fold_in(seeds[1], 2), own, number, TOK_DEV, EXPERTS, TOP, CAP, 2))(route_ids_keys, route_ids_turns).reshape((TOKENS, TOP))
    route_weight = jnp.clip(jnp.exp(math.log(1.0) - 2.3025851 * jax.random.uniform(seeds[2], (TOKENS, TOP), jnp.float32) ** level_of(seeds[2], (TOKENS, TOP), ((0, 64),), -0.2, 0.2)), 0.1, 1.0)
    expert_inputs = draw_expert_inputs(jax.random.fold_in(seeds[13], 71), 0)
    w_gate = centred(seeds[4], (EXPERTS, D, F), D ** -0.5, 0.125, ((0, 64), (2, 4)))
    w_up = centred(seeds[5], (EXPERTS, D, F), D ** -0.5, 0.125, ((0, 64), (2, 4)))
    w_down = centred(seeds[6], (EXPERTS, F, D), F ** -0.5, 0.1875, ((0, 64), (1, 4)))
    w_proj = centred(seeds[7], (D, D), D ** -0.5, 0.125, ((0, 4),))
    conv_out = centred(seeds[8], (TOKENS, D), 1.0, 6.0, ((0, 64), (1, 4)))
    channel_norm_gain = jnp.clip(1.0 + 0.18 * jax.random.normal(seeds[9], (D,), jnp.float32), 0.1, 1.9)
    taps = centred(seeds[10], (WIDTH, D), WIDTH ** -0.5, 1.0, ((1, 4),), jnp.float32)
    value_pre = centred(seeds[11], (TOKENS, D), 1.0, 6.0, ((0, 64), (1, 4)))
    gate_pre = centred(seeds[12], (TOKENS, D), 1.5, 6.0, ((0, 64), (1, 4)))
    return dict(cot_out=cot_out, route_ids=route_ids, route_weight=route_weight, expert_inputs=expert_inputs, w_gate=w_gate, w_up=w_up, w_down=w_down, w_proj=w_proj, conv_out=conv_out, channel_norm_gain=channel_norm_gain, taps=taps, value_pre=value_pre, gate_pre=gate_pre)


clamp_limit = 7.0
swish_alpha = 1.702
norm_epsilon = 1e-05

def one_expert(operands):
    rows_in, rows_cot, gate_weight, up_weight, down_weight = operands
    gate_lin = jnp.dot(rows_in, gate_weight, preferred_element_type=jnp.float32)
    up_lin = jnp.dot(rows_in, up_weight, preferred_element_type=jnp.float32)
    gate_c = jnp.minimum(gate_lin, clamp_limit)
    up_c = jnp.clip(up_lin, -clamp_limit, clamp_limit)
    sig = jax.nn.sigmoid(swish_alpha * gate_c)
    act = ((up_c + 1.0) * gate_c * sig).astype(jnp.bfloat16)
    grad_down = jnp.dot(act.T, rows_cot, preferred_element_type=jnp.float32).astype(jnp.bfloat16)
    d_act = jnp.dot(rows_cot, down_weight.T, preferred_element_type=jnp.float32)
    up_open = ((up_lin > -clamp_limit) & (up_lin < clamp_limit)).astype(jnp.float32)
    gate_open = (gate_lin < clamp_limit).astype(jnp.float32)
    d_up = (d_act * gate_c * sig * up_open).astype(jnp.bfloat16)
    d_gate = (d_act * (up_c + 1.0) * (sig + swish_alpha * gate_c * sig * (1.0 - sig)) * gate_open).astype(jnp.bfloat16)
    grad_gate = jnp.dot(rows_in.T, d_gate, preferred_element_type=jnp.float32).astype(jnp.bfloat16)
    grad_up = jnp.dot(rows_in.T, d_up, preferred_element_type=jnp.float32).astype(jnp.bfloat16)
    blocks = F // N_TP
    gate_parts = jnp.einsum('snf,dnf->nsd', d_gate.reshape(SLOTS, N_TP, blocks).astype(jnp.float32), gate_weight.reshape(D, N_TP, blocks).astype(jnp.float32))
    up_parts = jnp.einsum('snf,dnf->nsd', d_up.reshape(SLOTS, N_TP, blocks).astype(jnp.float32), up_weight.reshape(D, N_TP, blocks).astype(jnp.float32))
    rounded = (gate_parts + up_parts).astype(jnp.bfloat16)
    rounded = lax.optimization_barrier(rounded)
    input_grad = lax.optimization_barrier(jnp.sum(rounded.astype(jnp.float32), axis=0)).astype(jnp.bfloat16)
    return (grad_gate, grad_up, grad_down, input_grad)

def reference(cot_out, route_ids, route_weight, expert_inputs, w_gate, w_up, w_down, w_proj, conv_out, channel_norm_gain, taps, value_pre, gate_pre):
    block_ids = route_ids.reshape(N_SP, TOK_DEV * TOP)
    expert_hot = (block_ids[:, :, None] == jnp.arange(EXPERTS, dtype=jnp.int32)[None, None, :]).astype(jnp.int32)
    earlier = lax.optimization_barrier(jnp.sum((jnp.cumsum(expert_hot, axis=1) - expert_hot) * expert_hot, axis=2))
    dest_slot = (jnp.arange(N_SP, dtype=jnp.int32)[:, None] * CAP + earlier).reshape(-1).astype(jnp.int32)
    expert_of = block_ids.reshape(-1).astype(jnp.int32)
    repeated = jnp.repeat(cot_out, TOP, axis=0).astype(jnp.float32)
    scaled = (route_weight.reshape(-1)[:, None] * repeated).astype(jnp.bfloat16)
    expert_cot = jnp.zeros((EXPERTS, SLOTS, D), jnp.bfloat16).at[expert_of, dest_slot].set(scaled)
    grad_gate_w, grad_up_w, grad_down_w, expert_grad = lax.map(one_expert, (expert_inputs, expert_cot, w_gate, w_up, w_down))
    picked = expert_grad[expert_of, dest_slot].astype(jnp.float32).reshape(TOKENS, TOP, D)
    mix_grad = (cot_out.astype(jnp.float32) + lax.optimization_barrier(jnp.sum(picked, axis=1))).astype(jnp.bfloat16)
    convolution_filter = conv_out.astype(jnp.float32)
    channel_mean = lax.optimization_barrier(jnp.mean(convolution_filter, axis=1, keepdims=True))
    var = lax.optimization_barrier(jnp.mean(convolution_filter * convolution_filter, axis=1, keepdims=True)) - channel_mean * channel_mean
    inverse_deviation = lax.rsqrt(var + norm_epsilon)
    normalized_input = (convolution_filter - channel_mean) * inverse_deviation
    normalized_output = normalized_input * channel_norm_gain[None, :]
    sig = jax.nn.sigmoid(normalized_output)
    act_conv = (normalized_output * sig).astype(jnp.bfloat16)
    grad_proj = jnp.dot(act_conv.T, mix_grad, preferred_element_type=jnp.float32)
    d_act_conv = jnp.dot(mix_grad, w_proj.T, preferred_element_type=jnp.float32)
    normalized_gradient = d_act_conv * sig * (1.0 + normalized_output * (1.0 - sig)) * channel_norm_gain[None, :]
    first_moment_mean = lax.optimization_barrier(jnp.mean(normalized_gradient, axis=1, keepdims=True))
    second_moment_mean = lax.optimization_barrier(jnp.mean(normalized_gradient * normalized_input, axis=1, keepdims=True))
    convolution_gradient = inverse_deviation * (normalized_gradient - first_moment_mean - normalized_input * second_moment_mean)
    extended = jnp.concatenate([convolution_gradient, jnp.zeros((WIDTH - 1, D), jnp.float32)], axis=0)
    d_glu = jnp.zeros((TOKENS, D), jnp.float32)
    for offset in range(WIDTH):
        begin = WIDTH - 1 - offset
        d_glu = d_glu + taps[offset][None, :] * extended[begin:begin + TOKENS]
    gate_sig = jax.nn.sigmoid(gate_pre.astype(jnp.float32))
    grad_value = (d_glu * gate_sig).astype(jnp.bfloat16)
    grad_gate = (d_glu * value_pre.astype(jnp.float32) * gate_sig * (1.0 - gate_sig)).astype(jnp.bfloat16)
    return (grad_gate_w, grad_up_w, grad_down_w, grad_proj, grad_value, grad_gate)
```

```python
import jax
import jax.numpy as jnp
from jax import lax
from jax.experimental import pallas as pl
from jax.experimental.pallas import tpu as pltpu
from jax.sharding import Mesh
from jax.sharding import PartitionSpec as P

SP = ("sp_0", "sp_1", "sp_2")
ZX = ("sp_0", "sp_1")
CORE = "sp_2"
TP = "tp"
TP_SP = ("tp", "sp_0", "sp_1", "sp_2")

clamp_limit = 7.0
swish_alpha = 1.702
norm_epsilon = 1e-05
LANES = 128
bf16 = jnp.bfloat16
f32 = jnp.float32


def shifted(value, axis, steps):
    count = lax.axis_size(axis)
    return lax.ppermute(value, axis, [(i, (i + steps) % count) for i in range(count)])


def passed_along(value, axis, steps):
    count = lax.axis_size(axis)
    leading, last = (max(0, -steps), min(count, count - steps))
    return lax.ppermute(value, axis, [(source, source + steps) for source in range(leading, last)])


def dot(a, b, ca, cb):
    return lax.dot_general(a, b, (((ca,), (cb,)), ((), ())), preferred_element_type=f32)


def kernel(body, outs, *args, name, flops, scratch=(), smem=0):
    spaces = [pltpu.SMEM] * smem + [pltpu.VMEM] * (len(args) - smem)
    moved = sum(a.size * a.dtype.itemsize for a in (*args, *outs))
    return pl.pallas_call(
        body,
        out_shape=tuple(outs),
        in_specs=[pl.BlockSpec(memory_space=s) for s in spaces],
        out_specs=tuple(pl.BlockSpec(memory_space=pltpu.VMEM) for _ in outs),
        scratch_shapes=list(scratch),
        cost_estimate=pl.CostEstimate(flops=flops, transcendentals=0, bytes_accessed=moved),
        name=name,
    )(*args)


def struct(shape, dtype=bf16):
    return jax.ShapeDtypeStruct(shape, dtype)


def to_chunks(rows, scratch):
    n, parts = rows.shape[0], rows.shape[1] // LANES
    for j in range(parts):
        scratch[pl.ds(j, n, stride=parts), :] = rows[:, j * LANES : (j + 1) * LANES]


def from_chunks(chunks, scratch, n, parts):
    scratch[...] = chunks.astype(f32)
    pieces = [scratch[pl.ds(j, n, stride=parts), :].astype(bf16) for j in range(parts)]
    return jnp.concatenate(pieces, axis=1)


def dispatch_body(experts, capacity):
    def body(ids_ref, weight_ref, cot_ref, out_ref, dest_ref, scratch):
        tokens = ids_ref.shape[0]
        slots = experts * capacity
        id0, id1 = ids_ref[:, 0:1], ids_ref[:, 1:2]
        lane = lax.broadcasted_iota(jnp.int32, (tokens, LANES), 1)
        hot0 = (id0 == lane).astype(f32)
        hot1 = (id1 == lane).astype(f32)
        row = lax.broadcasted_iota(jnp.int32, (tokens, tokens), 0)
        col = lax.broadcasted_iota(jnp.int32, (tokens, tokens), 1)
        before = dot((row > col).astype(bf16), (hot0 + hot1).astype(bf16), 1, 0)
        slot0 = jnp.sum(before * hot0, axis=1, keepdims=True).astype(jnp.int32)
        slot1 = jnp.sum(before * hot1, axis=1, keepdims=True).astype(jnp.int32)
        dest0 = id0 * capacity + slot0
        dest1 = id1 * capacity + slot1
        dest_ref[:, 0:1] = dest0
        dest_ref[:, 1:2] = dest1
        place = lax.broadcasted_iota(jnp.int32, (tokens, slots), 1)
        spread = jnp.where(place == dest0, weight_ref[:, 0:1], 0.0) + jnp.where(
            place == dest1, weight_ref[:, 1:2], 0.0
        )
        high = spread.astype(bf16)
        low = (spread - high.astype(f32)).astype(bf16)
        cot = cot_ref[...]
        to_chunks(dot(high, cot, 0, 0) + dot(low, cot, 0, 0), scratch)
        out_ref[...] = scratch[...].astype(bf16)

    return body


def factors_body(rows_ref, gate_ref, up_ref, act_ref, for_up_ref, for_gate_ref):
    rows = rows_ref[...]
    gate_lin = dot(rows, gate_ref[...], 1, 0)
    up_lin = dot(rows, up_ref[...], 1, 0)
    gate_c = jnp.minimum(gate_lin, clamp_limit)
    up_c = jnp.clip(up_lin, -clamp_limit, clamp_limit)
    sigma = jax.nn.sigmoid(swish_alpha * gate_c)
    swish = gate_c * sigma
    act_ref[...] = ((up_c + 1.0) * swish).astype(bf16)
    up_open = (up_lin > -clamp_limit) & (up_lin < clamp_limit)
    for_up_ref[...] = jnp.where(up_open, swish, 0.0).astype(bf16)
    slope = (up_c + 1.0) * (sigma + swish_alpha * swish * (1.0 - sigma))
    for_gate_ref[...] = jnp.where(gate_lin < clamp_limit, slope, 0.0).astype(bf16)


def factors(rows_in, w_gate, w_up):
    rows, width = rows_in.shape
    hidden = w_gate.shape[1]
    block = rows // 3
    return pl.pallas_call(
        factors_body,
        grid=(3,),
        out_shape=(struct((rows, hidden)),) * 3,
        in_specs=[
            pl.BlockSpec((block, width), lambda i: (i, 0)),
            pl.BlockSpec((width, hidden), lambda i: (0, 0)),
            pl.BlockSpec((width, hidden), lambda i: (0, 0)),
        ],
        out_specs=(pl.BlockSpec((block, hidden), lambda i: (i, 0)),) * 3,
        cost_estimate=pl.CostEstimate(
            flops=4 * rows * width * hidden,
            transcendentals=rows * hidden,
            bytes_accessed=2 * (rows * width + 2 * width * hidden + 3 * rows * hidden),
        ),
        name="factors",
    )(rows_in, w_gate, w_up)


def partial_act_body(chunks_ref, far_ref, next_ref, prev_ref, own_ref, *outs_scratch):
    rows_ref, far_top, far_bot, next_top, next_bot, prev_top, prev_bot, own_out, scratch = outs_scratch
    n = rows_ref.shape[0]
    rows = from_chunks(chunks_ref[...], scratch, n, rows_ref.shape[1] // LANES)
    rows_ref[...] = rows
    half = n // 2
    for weight, top, bot in (
        (far_ref, far_top, far_bot),
        (next_ref, next_top, next_bot),
        (prev_ref, prev_top, prev_bot),
    ):
        value = dot(rows, weight[...], 1, 1).astype(bf16)
        top[...] = value[:half]
        bot[...] = value[half:]
    own_out[...] = dot(rows, own_ref[...], 1, 1).astype(bf16)


def block_of(ref, index, size):
    return ref[pl.ds(pl.multiple_of(index * size, size), size), :]


def hidden_grad_body(
    at_ref, own_ref, prev_top, near_top, next_bot, near_bot, up_ref, gate_ref, wg_ref, wu_ref,
    d_gate_ref, d_up_ref, far_top, far_bot,
):
    half = prev_top.shape[0]
    size = far_top.shape[1]
    count = wg_ref.shape[0] // size
    own = own_ref[...].astype(f32)
    top = own[:half] + prev_top[...].astype(f32) + near_top[...].astype(f32)
    bot = own[half:] + next_bot[...].astype(f32) + near_bot[...].astype(f32)
    d_act = jnp.concatenate([top, bot], axis=0)
    d_gate = (d_act * gate_ref[...].astype(f32)).astype(bf16)
    d_up = (d_act * up_ref[...].astype(f32)).astype(bf16)
    d_gate_ref[...] = d_gate
    d_up_ref[...] = d_up
    far = lax.rem(at_ref[0] + 2, count)
    value = dot(d_gate, block_of(wg_ref, far, size), 1, 1) + dot(d_up, block_of(wu_ref, far, size), 1, 1)
    value = value.astype(bf16)
    far_top[...] = value[:half]
    far_bot[...] = value[half:]


def input_grad_body(
    at_ref, d_gate_ref, d_up_ref, wg_ref, wu_ref, next_top, next_bot, prev_top, prev_bot, own_out
):
    half = next_top.shape[0]
    size = own_out.shape[1]
    count = wg_ref.shape[0] // size
    d_gate, d_up = d_gate_ref[...], d_up_ref[...]

    def part(shift):
        at = lax.rem(at_ref[0] + shift, count)
        value = dot(d_gate, block_of(wg_ref, at, size), 1, 1)
        value = value + dot(d_up, block_of(wu_ref, at, size), 1, 1)
        return value.astype(bf16)

    value = part(1)
    next_bot[...] = value[half:]
    next_top[...] = value[:half]
    value = part(count - 1)
    prev_top[...] = value[:half]
    prev_bot[...] = value[half:]
    own_out[...] = part(0)


def total_body(own_ref, prev_top, near_top, next_bot, near_bot, out_ref, scratch):
    half = prev_top.shape[0]
    own = own_ref[...].astype(f32)
    top = own[:half] + prev_top[...].astype(f32) + near_top[...].astype(f32)
    bot = own[half:] + next_bot[...].astype(f32) + near_bot[...].astype(f32)
    to_chunks(jnp.concatenate([top, bot], axis=0), scratch)
    out_ref[...] = scratch[...].astype(bf16)


def combine_body(chunks_ref, dest_ref, cot_ref, mix_ref, scratch):
    slots = scratch.shape[0] * LANES // cot_ref.shape[1]
    rows = from_chunks(chunks_ref[...], scratch, slots, cot_ref.shape[1] // LANES)
    tokens = cot_ref.shape[0]
    place = lax.broadcasted_iota(jnp.int32, (tokens, slots), 1)
    pick = (place == dest_ref[:, 0:1]) | (place == dest_ref[:, 1:2])
    summed = dot(pick.astype(f32).astype(bf16), rows, 1, 0)
    mix = (cot_ref[...].astype(f32) + summed).astype(bf16)
    for s in range(mix_ref.shape[0]):
        mix_ref[s] = mix


def down_grad_body(at_ref, act_ref, own_ref, next_ref, prev_ref, far_top, far_bot, out_ref):
    size = own_ref.shape[1]
    count = out_ref.shape[1] // size
    half = far_top.shape[0]
    act = act_ref[...]

    def put(shift, value):
        at = lax.rem(at_ref[0] + shift, count)
        out_ref[:, pl.ds(pl.multiple_of(at * size, size), size)] = value.astype(bf16)

    put(0, dot(act, own_ref[...], 0, 0))
    put(1, dot(act, next_ref[...], 0, 0))
    put(count - 1, dot(act, prev_ref[...], 0, 0))
    put(2, dot(act[:half], far_top[...], 0, 0) + dot(act[half:], far_bot[...], 0, 0))


def proj_grad_body(core_ref, act_ref, mix_ref, send_ref, keep_ref):
    count, _, size = mix_ref.shape
    rows = send_ref.shape[0]
    first = core_ref[0] == 0
    act = act_ref[...]
    for s in range(count):
        value = dot(act, mix_ref[s], 0, 0).reshape(rows // 8, 2, 8, size)
        zero, one = value[:, 0].reshape(rows, size), value[:, 1].reshape(rows, size)
        at = slice(s * size, (s + 1) * size)
        send_ref[:, at] = jnp.where(first, one, zero).astype(bf16)
        keep_ref[:, at] = jnp.where(first, zero, one).astype(bf16)


def reduce_over_ring(far_top, far_bot, rest):
    far_top_in = shifted(far_top, TP, 1)
    far_bot_in = shifted(far_bot, TP, -1)
    next_top, next_bot, prev_top, prev_bot, own = rest
    next_bot_in = shifted(next_bot, TP, 1)
    prev_top_in = shifted(prev_top, TP, -1)
    near_top = (next_top.astype(f32) + far_top_in.astype(f32)).astype(bf16)
    near_bot = (prev_bot.astype(f32) + far_bot_in.astype(f32)).astype(bf16)
    near_top_in = shifted(near_top, TP, 1)
    near_bot_in = shifted(near_bot, TP, -1)
    return own, prev_top_in, near_top_in, next_bot_in, near_bot_in


def per_device(
    cot_out,
    route_ids,
    route_weight,
    expert_inputs,
    w_gate,
    w_up,
    w_down,
    w_proj,
    conv_out,
    channel_norm_gain,
    taps,
    value_pre,
    gate_pre,
):
    experts = lax.axis_size(SP)
    ways = lax.axis_size(TP)
    tok_rows = cot_out.shape[0]
    slot_rows = expert_inputs.shape[1]
    capacity = slot_rows // experts
    local_cols = cot_out.shape[1]
    hidden = w_down.shape[1]
    half = slot_rows // 2
    parts = local_cols // LANES
    chunk_rows = slot_rows * parts
    at = lax.axis_index(TP)
    at_ref = at.reshape(1).astype(jnp.int32)
    core_ref = lax.axis_index(CORE).reshape(1).astype(jnp.int32)
    rows_in, gate_weight, up_weight, down_weight = expert_inputs[0], w_gate[0], w_up[0], w_down[0]
    chunk_scratch = pltpu.VMEM((chunk_rows, LANES), f32)

    outgoing, dest = kernel(
        dispatch_body(experts, capacity),
        (struct((chunk_rows, LANES)), struct((tok_rows, 2), jnp.int32)),
        route_ids, route_weight, cot_out,
        name="dispatch", flops=4 * tok_rows * slot_rows * local_cols, scratch=(chunk_scratch,),
    )
    moved = lax.all_to_all(
        outgoing.reshape(experts, chunk_rows // experts, LANES), SP, 0, 0, tiled=True
    )

    def down_block(shift):
        start = (at + shift) % ways * local_cols
        return lax.dynamic_slice_in_dim(down_weight, start, local_cols, 1)

    down_own = down_block(0)
    down_next = shifted(down_block(ways - 1), TP, -1)
    down_prev = shifted(down_block(1), TP, 1)
    down_far = shifted(down_block(2), TP, 2)
    act, for_up, for_gate = factors(rows_in, gate_weight, up_weight)

    conv_f = conv_out.astype(f32)
    channel_total = local_cols * ways
    first_sum, square_sum = lax.psum(
        (jnp.sum(conv_f, axis=1), jnp.sum(conv_f * conv_f, axis=1)), TP
    )

    rows_cot, far_top, far_bot, *rest = kernel(
        partial_act_body,
        (struct((slot_rows, local_cols)),) + (struct((half, hidden)),) * 6
        + (struct((slot_rows, hidden)),),
        moved.reshape(chunk_rows, LANES), down_far, down_next, down_prev, down_own,
        name="partial_act", flops=2 * slot_rows * local_cols * hidden * ways,
        scratch=(chunk_scratch,),
    )
    act_terms = reduce_over_ring(far_top, far_bot, rest)
    d_gate, d_up, far_top, far_bot = kernel(
        hidden_grad_body,
        (struct((slot_rows, hidden)),) * 2 + (struct((half, local_cols)),) * 2,
        at_ref, *act_terms, for_up, for_gate, gate_weight, up_weight,
        name="hidden_grad", flops=4 * slot_rows * local_cols * hidden, smem=1,
    )
    rest = kernel(
        input_grad_body,
        (struct((half, local_cols)),) * 4 + (struct((slot_rows, local_cols)),),
        at_ref, d_gate, d_up, gate_weight, up_weight,
        name="input_grad", flops=12 * slot_rows * local_cols * hidden, smem=1,
    )
    grad_terms = reduce_over_ring(far_top, far_bot, rest)
    (returning,) = kernel(
        total_body,
        (struct((chunk_rows, LANES)),),
        *grad_terms,
        name="total", flops=slot_rows * local_cols * 8, scratch=(chunk_scratch,),
    )
    coming = lax.all_to_all(
        returning.reshape(experts, chunk_rows // experts, LANES), SP, 0, 0, tiled=True
    )
    grad_gate_part = dot(rows_in, d_gate, 0, 0).astype(bf16)
    grad_up_part = dot(rows_in, d_up, 0, 0).astype(bf16)
    rows_cot, returning = lax.optimization_barrier((rows_cot, returning))
    rows_prev = shifted(rows_cot, TP, 1)
    rows_next = shifted(rows_cot, TP, -1)
    rows_far_top = shifted(rows_prev[:half], TP, 1)
    rows_far_bot = shifted(rows_next[half:], TP, -1)
    (grad_down,) = kernel(
        down_grad_body,
        (struct((hidden, local_cols * ways)),),
        at_ref, act, rows_cot, rows_next, rows_prev, rows_far_top, rows_far_bot,
        name="down_grad", flops=2 * slot_rows * hidden * local_cols * ways, smem=1,
    )

    (mix_copies,) = kernel(
        combine_body,
        (struct((ways, tok_rows, local_cols)),),
        coming.reshape(chunk_rows, LANES), dest, cot_out,
        name="combine", flops=2 * tok_rows * slot_rows * local_cols, scratch=(chunk_scratch,),
    )
    mix_full = lax.all_to_all(mix_copies, TP, 0, 0, tiled=True)

    channel_mean = (first_sum / channel_total)[:, None]
    var = (square_sum / channel_total)[:, None] - channel_mean * channel_mean
    inverse_deviation = lax.rsqrt(var + norm_epsilon)
    normalized_input = (conv_f - channel_mean) * inverse_deviation
    normalized_output = normalized_input * channel_norm_gain[None, :]
    sigma_conv = jax.nn.sigmoid(normalized_output)
    act_conv = (normalized_output * sigma_conv).astype(bf16)
    core_rows = local_cols // 2
    send, keep = kernel(
        proj_grad_body,
        (struct((core_rows, local_cols * ways)),) * 2,
        core_ref, act_conv, mix_full,
        name="proj_grad", flops=2 * tok_rows * local_cols * local_cols * ways, smem=1,
    )
    pair_sum = (keep.astype(f32) + shifted(send, CORE, 1).astype(f32)).astype(bf16)
    others = lax.axis_size(ZX)
    terms = lax.all_to_all(
        pair_sum.reshape(others, core_rows // others, local_cols * ways), ZX, 0, 0, tiled=True
    )
    grad_proj = jnp.sum(terms.astype(f32), axis=0)

    d_act_conv = sum(
        dot(mix_full[s], w_proj[:, s * local_cols : (s + 1) * local_cols], 1, 1) for s in range(ways)
    )
    normalized_gradient = (
        d_act_conv
        * sigma_conv
        * (1.0 + normalized_output * (1.0 - sigma_conv))
        * channel_norm_gain[None, :]
    )
    first_term, second_term = lax.psum(
        (
            jnp.sum(normalized_gradient, axis=1),
            jnp.sum(normalized_gradient * normalized_input, axis=1),
        ),
        TP,
    )
    convolution_gradient = inverse_deviation * (
        normalized_gradient
        - (first_term / channel_total)[:, None]
        - normalized_input * (second_term / channel_total)[:, None]
    )
    reach = taps.shape[0]
    following = passed_along(convolution_gradient[: reach - 1], SP, -1)
    extended = jnp.concatenate([convolution_gradient, following], axis=0)
    d_glu = jnp.zeros_like(convolution_gradient)
    for offset in range(reach):
        begin = reach - 1 - offset
        d_glu = d_glu + taps[offset][None, :] * extended[begin : begin + tok_rows]
    gate_sig = jax.nn.sigmoid(gate_pre.astype(f32))
    grad_value = (d_glu * gate_sig).astype(bf16)
    grad_gate = (d_glu * value_pre.astype(f32) * gate_sig * (1.0 - gate_sig)).astype(bf16)
    return (
        grad_gate_part[None],
        grad_up_part[None],
        grad_down[None],
        grad_proj,
        grad_value,
        grad_gate,
    )


def solution(mesh):
    finer = Mesh(mesh.devices.reshape(8, 4, 2, mesh.shape["tp"]), ("sp_0", "sp_1", "sp_2", "tp"))
    placed = (
        P(SP, "tp"),
        P(SP, None),
        P(SP, None),
        P(SP, None, None),
        P(SP, None, "tp"),
        P(SP, None, "tp"),
        P(SP, "tp", None),
        P("tp", None),
        P(SP, "tp"),
        P("tp"),
        P(None, "tp"),
        P(SP, "tp"),
        P(SP, "tp"),
    )
    return jax.shard_map(
        per_device,
        mesh=finer,
        in_specs=placed,
        out_specs=(
            P(SP, None, "tp"),
            P(SP, None, "tp"),
            P(SP, "tp", None),
            P(TP_SP, None),
            P(SP, "tp"),
            P(SP, "tp"),
        ),
        check_vma=False,
    )
```

```python
import jax
import jax.numpy as jnp
from jax import lax
from jax.experimental import pallas as pl
from jax.experimental.pallas import tpu as pltpu
from jax.sharding import Mesh
from jax.sharding import PartitionSpec as P

SP = ("sp_0", "sp_1", "sp_2")
ZX = ("sp_0", "sp_1")
CORE = "sp_2"
TP = "tp"
TP_SP = ("tp", "sp_0", "sp_1", "sp_2")

clamp_limit = 7.0
swish_alpha = 1.702
norm_epsilon = 1e-05
LANES = 128
bf16 = jnp.bfloat16
f32 = jnp.float32


def shifted(value, axis, steps):
    count = lax.axis_size(axis)
    return lax.ppermute(value, axis, [(i, (i + steps) % count) for i in range(count)])


def passed_along(value, axis, steps):
    count = lax.axis_size(axis)
    leading, last = (max(0, -steps), min(count, count - steps))
    return lax.ppermute(value, axis, [(source, source + steps) for source in range(leading, last)])


def dot(a, b, ca, cb):
    return lax.dot_general(a, b, (((ca,), (cb,)), ((), ())), preferred_element_type=f32)


def kernel(body, outs, *args, flops, scratch=(), smem=0, limit=24, staged=True, to_hbm=()):
    spaces = [pltpu.SMEM] * smem + [pltpu.VMEM] * (len(args) - smem)
    moved = sum(a.size * a.dtype.itemsize for a in (*args[smem:], *outs))
    place = pltpu.VMEM if staged else pltpu.HBM
    args = args[:smem] + tuple(pltpu.with_memory_space_constraint(a, place) for a in args[smem:])
    return pl.pallas_call(
        body,
        out_shape=tuple(
            (pltpu.HBM if i in to_hbm else pltpu.VMEM)(o.shape, o.dtype) for i, o in enumerate(outs)
        ),
        in_specs=[pl.BlockSpec(memory_space=s) for s in spaces],
        out_specs=tuple(pl.BlockSpec(memory_space=pltpu.VMEM) for _ in outs),
        scratch_shapes=list(scratch),
        cost_estimate=pl.CostEstimate(flops=flops, transcendentals=0, bytes_accessed=moved),
        compiler_params=pltpu.CompilerParams(vmem_limit_bytes=limit << 20),
    )(*args)


def struct(shape, dtype=bf16):
    return jax.ShapeDtypeStruct(shape, dtype)


def to_chunks(rows, scratch):
    n, parts = rows.shape[0], rows.shape[1] // LANES
    for j in range(parts):
        scratch[pl.ds(j, n, stride=parts), :] = rows[:, j * LANES : (j + 1) * LANES]


def from_chunks(chunks, scratch, n, parts):
    scratch[...] = chunks.astype(f32)
    pieces = [scratch[pl.ds(j, n, stride=parts), :].astype(bf16) for j in range(parts)]
    return jnp.concatenate(pieces, axis=1)


def dispatch_body(experts, capacity):
    def body(ids_ref, weight_ref, cot_ref, out_ref, dest_ref, scratch):
        tokens = ids_ref.shape[1]
        slots = experts * capacity
        id0, id1 = ids_ref[0:1, :], ids_ref[1:2, :]
        expert = lax.broadcasted_iota(jnp.int32, (LANES, tokens), 0)
        hot0 = (id0 == expert).astype(f32)
        hot1 = (id1 == expert).astype(f32)
        row = lax.broadcasted_iota(jnp.int32, (tokens, tokens), 0)
        col = lax.broadcasted_iota(jnp.int32, (tokens, tokens), 1)
        before = dot((hot0 + hot1).astype(bf16), (row < col).astype(f32).astype(bf16), 1, 0)
        slot0 = jnp.sum(before * hot0, axis=0, keepdims=True).astype(jnp.int32)
        slot1 = jnp.sum(before * hot1, axis=0, keepdims=True).astype(jnp.int32)
        dest0 = id0 * capacity + slot0
        dest1 = id1 * capacity + slot1
        dest_ref[0:1, :] = dest0
        dest_ref[1:2, :] = dest1
        place = lax.broadcasted_iota(jnp.int32, (slots, tokens), 0)
        spread = jnp.where(place == dest0, weight_ref[0:1, :], 0.0) + jnp.where(
            place == dest1, weight_ref[1:2, :], 0.0
        )
        high = spread.astype(bf16)
        low = (spread - high.astype(f32)).astype(bf16)
        cot = cot_ref[...]
        to_chunks(dot(high, cot, 1, 0) + dot(low, cot, 1, 0), scratch)
        out_ref[...] = scratch[...].astype(bf16)

    return body


def pick_body(dest_ref, pick_ref):
    tokens, slots = pick_ref.shape
    row = lax.broadcasted_iota(jnp.int32, (tokens, tokens), 0)
    col = lax.broadcasted_iota(jnp.int32, (tokens, tokens), 1)
    dest0, dest1 = (
        jnp.sum(jnp.where(row == col, dest_ref[k : k + 1, :].astype(f32), 0.0), axis=1, keepdims=True)
        .astype(jnp.int32)
        for k in range(2)
    )
    place = lax.broadcasted_iota(jnp.int32, (tokens, slots), 1)
    pick_ref[...] = ((place == dest0) | (place == dest1)).astype(f32).astype(bf16)


def factors_body(rows_ref, gate_ref, up_ref, act_ref, for_up_ref, for_gate_ref):
    block = rows_ref.shape[0] // 3

    def step(i, _):
        at = pl.ds(pl.multiple_of(i * block, block), block)
        rows = rows_ref[at, :]
        gate_lin = dot(rows, gate_ref[...], 1, 0)
        up_lin = dot(rows, up_ref[...], 1, 0)
        gate_c = jnp.minimum(gate_lin, clamp_limit)
        up_c = jnp.clip(up_lin, -clamp_limit, clamp_limit)
        sigma = jax.nn.sigmoid(swish_alpha * gate_c)
        swish = gate_c * sigma
        act_ref[at, :] = ((up_c + 1.0) * swish).astype(bf16)
        up_open = (up_lin > -clamp_limit) & (up_lin < clamp_limit)
        for_up_ref[at, :] = jnp.where(up_open, swish, 0.0).astype(bf16)
        slope = (up_c + 1.0) * (sigma + swish_alpha * swish * (1.0 - sigma))
        for_gate_ref[at, :] = jnp.where(gate_lin < clamp_limit, slope, 0.0).astype(bf16)
        return 0

    lax.fori_loop(0, 3, step, 0)


def partial_act_body(chunks_ref, far_ref, next_ref, prev_ref, own_ref, *outs_scratch):
    rows_top, rows_bot, *outs, own_out, scratch = outs_scratch
    far_top, far_bot, next_top, next_bot, prev_top, prev_bot = outs
    half, width = rows_top.shape
    rows = from_chunks(chunks_ref[...], scratch, 2 * half, width // LANES)
    rows_top[...] = rows[:half]
    rows_bot[...] = rows[half:]
    for weight, top, bot in (
        (far_ref, far_top, far_bot),
        (next_ref, next_top, next_bot),
        (prev_ref, prev_top, prev_bot),
    ):
        value = dot(rows, weight[...], 1, 1).astype(bf16)
        top[...] = value[:half]
        bot[...] = value[half:]
    own_out[...] = dot(rows, own_ref[...], 1, 1).astype(bf16)


def block_of(ref, index, size):
    return ref[pl.ds(pl.multiple_of(index * size, size), size), :]


def hidden_grad_body(
    at_ref, own_ref, prev_top, near_top, next_bot, near_bot, up_ref, gate_ref, wg_ref, wu_ref,
    d_gate_ref, d_up_ref, far_top, far_bot,
):
    half = prev_top.shape[0]
    size = far_top.shape[1]
    count = wg_ref.shape[0] // size
    own = own_ref[...].astype(f32)
    top = own[:half] + prev_top[...].astype(f32) + near_top[...].astype(f32)
    bot = own[half:] + next_bot[...].astype(f32) + near_bot[...].astype(f32)
    d_act = jnp.concatenate([top, bot], axis=0)
    d_gate = (d_act * gate_ref[...].astype(f32)).astype(bf16)
    d_up = (d_act * up_ref[...].astype(f32)).astype(bf16)
    d_gate_ref[...] = d_gate
    d_up_ref[...] = d_up
    far = lax.rem(at_ref[0] + 2, count)
    value = dot(d_gate, block_of(wg_ref, far, size), 1, 1) + dot(d_up, block_of(wu_ref, far, size), 1, 1)
    value = value.astype(bf16)
    far_top[...] = value[:half]
    far_bot[...] = value[half:]


def input_grad_body(
    at_ref, d_gate_ref, d_up_ref, wg_ref, wu_ref, next_top, next_bot, prev_top, prev_bot, own_out
):
    half = next_top.shape[0]
    size = own_out.shape[1]
    count = wg_ref.shape[0] // size
    d_gate, d_up = d_gate_ref[...], d_up_ref[...]

    def part(shift):
        at = lax.rem(at_ref[0] + shift, count)
        value = dot(d_gate, block_of(wg_ref, at, size), 1, 1)
        value = value + dot(d_up, block_of(wu_ref, at, size), 1, 1)
        return value.astype(bf16)

    value = part(1)
    next_bot[...] = value[half:]
    next_top[...] = value[:half]
    value = part(count - 1)
    prev_top[...] = value[:half]
    prev_bot[...] = value[half:]
    own_out[...] = part(0)


def total_body(own_ref, prev_top, near_top, next_bot, near_bot, out_ref, scratch):
    half = prev_top.shape[0]
    own = own_ref[...].astype(f32)
    top = own[:half] + prev_top[...].astype(f32) + near_top[...].astype(f32)
    bot = own[half:] + next_bot[...].astype(f32) + near_bot[...].astype(f32)
    to_chunks(jnp.concatenate([top, bot], axis=0), scratch)
    out_ref[...] = scratch[...].astype(bf16)


def combine_body(chunks_ref, pick_ref, cot_ref, mix_ref, scratch):
    slots = pick_ref.shape[1]
    rows = from_chunks(chunks_ref[...], scratch, slots, cot_ref.shape[1] // LANES)
    mix_ref[...] = (cot_ref[...].astype(f32) + dot(pick_ref[...], rows, 1, 0)).astype(bf16)


def down_grad_body(at_ref, act_ref, *refs):
    *rows, out_ref = refs
    half, size = rows[0].shape
    count = out_ref.shape[1] // size
    for i, shift in enumerate((0, 1, count - 1, 2)):
        top, bot = rows[2 * i : 2 * i + 2]
        value = dot(act_ref[:half, :], top[...], 0, 0) + dot(act_ref[half:, :], bot[...], 0, 0)
        at = lax.rem(at_ref[0] + shift, count)
        out_ref[:, pl.ds(pl.multiple_of(at * size, size), size)] = value.astype(bf16)


def proj_grad_body(core_ref, act_ref, *mix_refs):
    *mixes, send_ref, keep_ref = mix_refs
    rows, size = send_ref.shape[0], act_ref.shape[1]
    first = core_ref[0] == 0
    act = act_ref[...]
    for s, mix_ref in enumerate(mixes):
        value = dot(act, mix_ref[...], 0, 0).reshape(rows // 8, 2, 8, size)
        zero, one = value[:, 0].reshape(rows, size), value[:, 1].reshape(rows, size)
        at = slice(s * size, (s + 1) * size)
        send_ref[:, at] = jnp.where(first, one, zero).astype(bf16)
        keep_ref[:, at] = jnp.where(first, zero, one).astype(bf16)


def pair_sum_body(near_ref, near_in_ref, far_ref, far_in_ref, out_ref):
    near = near_ref.shape[1]
    out_ref[:, :near] = (near_ref[...].astype(f32) + near_in_ref[...].astype(f32)).astype(bf16)
    out_ref[:, near:] = (far_ref[...].astype(f32) + far_in_ref[...].astype(f32)).astype(bf16)


def proj_total_body(count):
    def body(at_ref, terms_ref, out_ref):
        rows, width = out_ref.shape
        terms = terms_ref[...].astype(f32)
        total = jnp.sum(terms.reshape(terms.shape[0] // rows, rows, width), axis=0)
        size = width // count
        for s, shift in enumerate((0, 1, count - 1, 2)):
            at = lax.rem(at_ref[0] + shift, count)
            out_ref[:, pl.ds(pl.multiple_of(at * size, size), size)] = total[
                :, s * size : (s + 1) * size
            ]

    return body


def split(value, pieces):
    terms = []
    for _ in range(pieces):
        terms.append(value.astype(bf16))
        value = value - terms[-1].astype(f32)
    return terms


def row_sums(first, second, out_ref):
    ones = jnp.ones((8, first.shape[1]), bf16)
    one = sum(dot(ones, term, 1, 1) for term in split(first, 3))
    two = sum(dot(ones, term, 1, 1) for term in split(second, 3))
    row = lax.broadcasted_iota(jnp.int32, out_ref.shape, 0)
    out_ref[...] = jnp.where(row == 0, one, jnp.where(row == 1, two, 0.0))


def along_rows(sums, index):
    row = lax.broadcasted_iota(jnp.int32, (8, LANES), 0)
    chosen = (row == index).astype(f32).astype(bf16)
    return sum(dot(term, chosen, 0, 0) for term in split(sums, 3))


def widened(value, lanes):
    return jnp.concatenate([value] * (lanes // LANES), axis=1)


def stats_body(conv_ref, out_ref):
    conv = conv_ref[...].astype(f32)
    row_sums(conv, conv * conv, out_ref)


def norm_body(channels):
    def body(own, one, two, three, conv_ref, gain_ref, act_ref, xhat_ref, slope_ref, rstd_ref):
        sums = own[...] + one[...] + two[...] + three[...]
        width = conv_ref.shape[1]
        mean = along_rows(sums, 0) / channels
        var = along_rows(sums, 1) / channels - mean * mean
        rstd = lax.rsqrt(var + norm_epsilon)
        rstd_ref[...] = rstd
        xhat = (conv_ref[...].astype(f32) - widened(mean, width)) * widened(rstd, width)
        gain = gain_ref[...]
        normed = xhat * gain
        sigma = jax.nn.sigmoid(normed)
        act_ref[...] = (normed * sigma).astype(bf16)
        xhat_ref[...] = xhat
        slope_ref[...] = sigma * (1.0 + normed * (1.0 - sigma)) * gain

    return body


def norm_grad_body(at_ref, own, following, previous, far, proj_ref, xhat_ref, slope_ref, dxh_ref, sums_ref):
    size = own.shape[1]
    count = proj_ref.shape[1] // size
    value = None
    for shift, mix_ref in ((0, own), (1, following), (count - 1, previous), (2, far)):
        at = lax.rem(at_ref[0] + shift, count)
        weight = proj_ref[:, pl.ds(pl.multiple_of(at * size, size), size)]
        term = dot(mix_ref[...], weight, 1, 1)
        value = term if value is None else value + term
    dxh = value * slope_ref[...]
    dxh_ref[...] = dxh
    row_sums(dxh, dxh * xhat_ref[...], sums_ref)


def conv_grad_body(channels):
    def body(own, one, two, three, dxh_ref, xhat_ref, rstd_ref, out_ref, edge_ref):
        sums = own[...] + one[...] + two[...] + three[...]
        width = dxh_ref.shape[1]
        first = widened(along_rows(sums, 0) / channels, width)
        second = widened(along_rows(sums, 1) / channels, width)
        value = widened(rstd_ref[...], width) * (dxh_ref[...] - first - xhat_ref[...] * second)
        out_ref[...] = value
        edge_ref[...] = value[: edge_ref.shape[0]]

    return body


def conv_body(grad_ref, edge_ref, taps_ref, value_ref, gate_ref, value_out, gate_out, extended):
    tokens, width = grad_ref.shape
    reach = taps_ref.shape[0]
    extended[:tokens, :] = grad_ref[...]
    extended[tokens:, :] = edge_ref[...]
    block = 64

    def step(i, _):
        lanes = pl.ds(pl.multiple_of(i * LANES, LANES), LANES)
        for start in range(0, tokens, block):
            total = jnp.zeros((block, LANES), f32)
            for offset in range(reach):
                tap = taps_ref[reach - 1 - offset : reach - offset, lanes]
                total = total + tap * extended[start + offset : start + offset + block, lanes]
            rows = slice(start, start + block)
            sigma = jax.nn.sigmoid(gate_ref[rows, lanes].astype(f32))
            scaled = total * sigma
            value_out[rows, lanes] = scaled.astype(bf16)
            gate = scaled * value_ref[rows, lanes].astype(f32) * (1.0 - sigma)
            gate_out[rows, lanes] = gate.astype(bf16)
        return 0

    lax.fori_loop(0, width // LANES, step, 0)


def weight_grad_body(rows_ref, gate_ref, up_ref, gate_out, up_out):
    size = gate_ref.shape[1]
    both = jnp.concatenate([gate_ref[...], up_ref[...]], axis=1)

    def step(i, _):
        at = pl.ds(pl.multiple_of(i * size, size), size)
        value = dot(rows_ref[:, at], both, 0, 0)
        gate_out[at, :] = value[:, :size].astype(bf16)
        up_out[at, :] = value[:, size:].astype(bf16)
        return 0

    lax.fori_loop(0, rows_ref.shape[1] // size, step, 0)


def near_body(one_ref, two_ref, out_ref):
    out_ref[...] = (one_ref[...].astype(f32) + two_ref[...].astype(f32)).astype(bf16)


def near_sum(one, two):
    (value,) = kernel(near_body, (struct(one.shape),), one, two, flops=one.size, limit=4)
    return value


def exchanged(value):
    return shifted(value, TP, 1), shifted(value, TP, -1), shifted(value, TP, 2)


def reduce_over_ring(far_top, far_bot, rest):
    far_top_in = shifted(far_top, TP, 1)
    far_bot_in = shifted(far_bot, TP, -1)
    next_top, next_bot, prev_top, prev_bot, own = rest
    next_bot_in = shifted(next_bot, TP, 1)
    prev_top_in = shifted(prev_top, TP, -1)
    near_top = near_sum(next_top, far_top_in)
    near_bot = near_sum(prev_bot, far_bot_in)
    near_top_in = shifted(near_top, TP, 1)
    near_bot_in = shifted(near_bot, TP, -1)
    return own, prev_top_in, near_top_in, next_bot_in, near_bot_in


def per_device(
    cot_out,
    route_ids,
    route_weight,
    expert_inputs,
    w_gate,
    w_up,
    w_down,
    w_proj,
    conv_out,
    channel_norm_gain,
    taps,
    value_pre,
    gate_pre,
):
    experts = lax.axis_size(SP)
    ways = lax.axis_size(TP)
    tok_rows = cot_out.shape[0]
    slot_rows = expert_inputs.shape[1]
    capacity = slot_rows // experts
    local_cols = cot_out.shape[1]
    hidden = w_down.shape[1]
    half = slot_rows // 2
    parts = local_cols // LANES
    chunk_rows = slot_rows * parts
    at = lax.axis_index(TP)
    at_ref = at.reshape(1).astype(jnp.int32)
    core_ref = lax.axis_index(CORE).reshape(1).astype(jnp.int32)
    rows_in, gate_weight, up_weight, down_weight = expert_inputs[0], w_gate[0], w_up[0], w_down[0]
    chunk_scratch = pltpu.VMEM((chunk_rows, LANES), f32)

    outgoing, dest = kernel(
        dispatch_body(experts, capacity),
        (struct((chunk_rows, LANES)), struct((2, tok_rows), jnp.int32)),
        route_ids.T, route_weight.T, cot_out,
        flops=4 * tok_rows * slot_rows * local_cols, scratch=(chunk_scratch,),
        staged=False, to_hbm=(0, 1),
    )
    moved = lax.all_to_all(
        outgoing.reshape(experts, chunk_rows // experts, LANES), SP, 0, 0, tiled=True
    )
    dest, conv_late, down_late = lax.optimization_barrier((dest, conv_out, down_weight))

    def down_block(shift):
        start = (at + shift) % ways * local_cols
        return lax.dynamic_slice_in_dim(down_late, start, local_cols, 1)

    down_own = down_block(0)
    down_next = shifted(down_block(ways - 1), TP, -1)
    down_prev = shifted(down_block(1), TP, 1)
    down_far = shifted(down_block(2), TP, 2)
    act, for_up, for_gate = kernel(
        factors_body,
        (struct((slot_rows, hidden)),) * 3,
        rows_in, gate_weight, up_weight,
        flops=4 * slot_rows * hidden * local_cols * ways,
    )
    (pick,) = kernel(
        pick_body, (struct((tok_rows, slot_rows)),), dest, flops=tok_rows * slot_rows * 8
    )
    channel_total = local_cols * ways
    tokens_8 = struct((8, tok_rows), f32)
    block = struct((tok_rows, local_cols), f32)
    (stats,) = kernel(stats_body, (tokens_8,), conv_late, flops=48 * tok_rows * local_cols, limit=8)
    stats_in = exchanged(stats)
    moved, act, for_up, for_gate, pick, stats_in = lax.optimization_barrier(
        (moved, act, for_up, for_gate, pick, stats_in)
    )

    rows_top, rows_bot, far_top, far_bot, *rest = kernel(
        partial_act_body,
        (struct((half, local_cols)),) * 2 + (struct((half, hidden)),) * 6
        + (struct((slot_rows, hidden)),),
        moved.reshape(chunk_rows, LANES), down_far, down_next, down_prev, down_own,
        flops=2 * slot_rows * local_cols * hidden * ways,
        scratch=(chunk_scratch,), to_hbm=(0, 1),
    )
    act_terms = reduce_over_ring(far_top, far_bot, rest)
    d_gate, d_up, far_top, far_bot = kernel(
        hidden_grad_body,
        (struct((slot_rows, hidden)),) * 2 + (struct((half, local_cols)),) * 2,
        at_ref, *act_terms, for_up, for_gate, gate_weight, up_weight,
        flops=4 * slot_rows * local_cols * hidden, smem=1,
    )
    rest = kernel(
        input_grad_body,
        (struct((half, local_cols)),) * 4 + (struct((slot_rows, local_cols)),),
        at_ref, d_gate, d_up, gate_weight, up_weight,
        flops=12 * slot_rows * local_cols * hidden, smem=1,
    )
    grad_terms = reduce_over_ring(far_top, far_bot, rest)
    (returning,) = kernel(
        total_body,
        (struct((chunk_rows, LANES)),),
        *grad_terms,
        flops=slot_rows * local_cols * 8, scratch=(chunk_scratch,),
    )
    coming = lax.all_to_all(
        returning.reshape(experts, chunk_rows // experts, LANES), SP, 0, 0, tiled=True
    )
    grad_gate_part, grad_up_part = kernel(
        weight_grad_body,
        (struct((local_cols * ways, hidden)),) * 2,
        rows_in, d_gate, d_up,
        flops=4 * slot_rows * hidden * local_cols * ways, to_hbm=(0, 1),
    )
    rows_top, rows_bot, _ = lax.optimization_barrier((rows_top, rows_bot, returning))
    prev_top = shifted(rows_top, TP, 1)
    next_bot = shifted(rows_bot, TP, -1)
    prev_bot = shifted(rows_bot, TP, 1)
    next_top = shifted(rows_top, TP, -1)
    coming, grad_gate_part, grad_up_part = lax.optimization_barrier(
        (coming, grad_gate_part, grad_up_part)
    )
    (mix,) = kernel(
        combine_body,
        (struct((tok_rows, local_cols)),),
        coming.reshape(chunk_rows, LANES), pick, cot_out,
        flops=2 * tok_rows * slot_rows * local_cols, scratch=(chunk_scratch,),
    )
    mix_far = shifted(mix, TP, 2)
    mix_prev = shifted(mix, TP, 1)
    mix_next = shifted(mix, TP, -1)
    conv_last, _ = lax.optimization_barrier((conv_out, mix))
    act_conv, xhat, slope, rstd = kernel(
        norm_body(channel_total),
        (struct((tok_rows, local_cols)), block, block, struct((tok_rows, LANES), f32)),
        stats, *stats_in, conv_last, channel_norm_gain.reshape(1, local_cols),
        flops=20 * tok_rows * local_cols, limit=8,
    )
    core_rows = local_cols // 2
    near = (ways - 1) * local_cols
    send, keep = kernel(
        proj_grad_body,
        (struct((core_rows, near)),) * 2,
        core_ref, act_conv, mix, mix_next, mix_prev,
        flops=6 * tok_rows * local_cols * local_cols, smem=1,
    )
    came = shifted(send, CORE, 1)
    send_far, keep_far = kernel(
        proj_grad_body,
        (struct((core_rows, local_cols)),) * 2,
        core_ref, act_conv, mix_far,
        flops=2 * tok_rows * local_cols * local_cols, smem=1,
    )
    came_far = shifted(send_far, CORE, 1)
    dxh, sums = kernel(
        norm_grad_body,
        (block, tokens_8),
        at_ref, mix, mix_next, mix_prev, mix_far, w_proj, xhat, slope,
        flops=2 * tok_rows * local_cols * local_cols * ways, smem=1,
    )
    came_far, dxh, sums = lax.optimization_barrier((came_far, dxh, sums))
    (pair_sum,) = kernel(
        pair_sum_body,
        (struct((core_rows, local_cols * ways)),),
        keep, came, keep_far, came_far,
        flops=core_rows * local_cols * ways, limit=8,
    )
    others = lax.axis_size(ZX)
    terms = lax.all_to_all(
        pair_sum.reshape(others, core_rows // others, local_cols * ways), ZX, 0, 0, tiled=True
    )
    (grad_proj,) = kernel(
        proj_total_body(ways),
        (struct((core_rows // others, local_cols * ways), f32),),
        at_ref, terms.reshape(core_rows, local_cols * ways),
        flops=core_rows * local_cols * ways, smem=1, limit=8, to_hbm=(0,),
    )
    sums, _ = lax.optimization_barrier((sums, pair_sum))
    sums_in = exchanged(sums)
    rows_far_top = shifted(prev_top, TP, 1)
    rows_far_bot = shifted(next_bot, TP, -1)
    (grad_down,) = kernel(
        down_grad_body,
        (struct((hidden, local_cols * ways)),),
        at_ref, act, rows_top, rows_bot, next_top, next_bot, prev_top, prev_bot, rows_far_top, rows_far_bot,
        flops=2 * slot_rows * hidden * local_cols * ways, smem=1, to_hbm=(0,),
    )
    reach = taps.shape[0]
    convolution_gradient, edge = kernel(
        conv_grad_body(channel_total),
        (block, struct((32, local_cols), f32)),
        sums, *sums_in, dxh, xhat, rstd,
        flops=8 * tok_rows * local_cols, limit=8,
    )
    following = passed_along(edge, SP, -1)
    following, grad_down = lax.optimization_barrier((following, grad_down))
    grad_value, grad_gate = kernel(
        conv_body,
        (struct((tok_rows, local_cols)),) * 2,
        convolution_gradient, following, taps, value_pre, gate_pre,
        flops=2 * reach * tok_rows * local_cols, limit=8, to_hbm=(0, 1),
        scratch=(pltpu.VMEM((tok_rows + edge.shape[0], local_cols), f32),),
    )
    return (
        grad_gate_part[None],
        grad_up_part[None],
        grad_down[None],
        grad_proj,
        grad_value,
        grad_gate,
    )


def solution(mesh):
    finer = Mesh(mesh.devices.reshape(8, 4, 2, mesh.shape["tp"]), ("sp_0", "sp_1", "sp_2", "tp"))
    placed = (
        P(SP, "tp"),
        P(SP, None),
        P(SP, None),
        P(SP, None, None),
        P(SP, None, "tp"),
        P(SP, None, "tp"),
        P(SP, "tp", None),
        P("tp", None),
        P(SP, "tp"),
        P("tp"),
        P(None, "tp"),
        P(SP, "tp"),
        P(SP, "tp"),
    )

    return jax.shard_map(
        per_device,
        mesh=finer,
        in_specs=placed,
        out_specs=(
            P(SP, None, "tp"),
            P(SP, None, "tp"),
            P(SP, "tp", None),
            P(TP_SP, None),
            P(SP, "tp"),
            P(SP, "tp"),
        ),
        check_vma=False,
    )
```

```python
import jax
import jax.numpy as jnp
from jax import lax
from jax.experimental import pallas as pl
from jax.experimental.pallas import tpu as pltpu
from jax.sharding import Mesh
from jax.sharding import PartitionSpec as P

SP = ("sp_0", "sp_1", "sp_2")
PLANE = "sp_0"
COLUMN = "sp_1"
CORE = "sp_2"
TP = "tp"
TP_SP = ("tp", "sp_0", "sp_1", "sp_2")

clamp_limit = 7.0
swish_alpha = 1.702
norm_epsilon = 1e-05
LANES = 128
bf16 = jnp.bfloat16
f32 = jnp.float32


def shifted(value, axis, steps):
    count = lax.axis_size(axis)
    return lax.ppermute(value, axis, [(i, (i + steps) % count) for i in range(count)])


def passed_along(value, axis, steps):
    count = lax.axis_size(axis)
    leading, last = (max(0, -steps), min(count, count - steps))
    return lax.ppermute(value, axis, [(source, source + steps) for source in range(leading, last)])


def dot(a, b, ca, cb):
    return lax.dot_general(a, b, (((ca,), (cb,)), ((), ())), preferred_element_type=f32)


def kernel(body, outs, *args, flops, scratch=(), smem=0, limit=24, staged=range(99), to_hbm=()):
    spaces = [pltpu.SMEM] * smem + [pltpu.VMEM] * (len(args) - smem)
    moved = sum(a.size * a.dtype.itemsize for a in (*args[smem:], *outs))
    args = args[:smem] + tuple(
        pltpu.with_memory_space_constraint(a, pltpu.VMEM if i in staged else pltpu.HBM)
        for i, a in enumerate(args[smem:])
    )
    return pl.pallas_call(
        body,
        out_shape=tuple(
            (pltpu.HBM if i in to_hbm else pltpu.VMEM)(o.shape, o.dtype) for i, o in enumerate(outs)
        ),
        in_specs=[pl.BlockSpec(memory_space=s) for s in spaces],
        out_specs=tuple(pl.BlockSpec(memory_space=pltpu.VMEM) for _ in outs),
        scratch_shapes=list(scratch),
        cost_estimate=pl.CostEstimate(flops=flops, transcendentals=0, bytes_accessed=moved),
        compiler_params=pltpu.CompilerParams(vmem_limit_bytes=limit << 20),
    )(*args)


def struct(shape, dtype=bf16):
    return jax.ShapeDtypeStruct(shape, dtype)


def to_chunks(rows, scratch):
    n, parts = rows.shape[0], rows.shape[1] // LANES
    for j in range(parts):
        scratch[pl.ds(j, n, stride=parts), :] = rows[:, j * LANES : (j + 1) * LANES]


def from_chunks(chunks, scratch, n, parts):
    scratch[...] = chunks.astype(f32)
    pieces = [scratch[pl.ds(j, n, stride=parts), :].astype(bf16) for j in range(parts)]
    return jnp.concatenate(pieces, axis=1)


def dispatch_body(experts, capacity):
    def body(ids_ref, weight_ref, cot_ref, out_ref, dest_ref, scratch):
        tokens = ids_ref.shape[1]
        slots = experts * capacity
        id0, id1 = ids_ref[0:1, :], ids_ref[1:2, :]
        expert = lax.broadcasted_iota(jnp.int32, (LANES, tokens), 0)
        hot0 = (id0 == expert).astype(f32)
        hot1 = (id1 == expert).astype(f32)
        row = lax.broadcasted_iota(jnp.int32, (tokens, tokens), 0)
        col = lax.broadcasted_iota(jnp.int32, (tokens, tokens), 1)
        before = dot((hot0 + hot1).astype(bf16), (row < col).astype(f32).astype(bf16), 1, 0)
        slot0 = jnp.sum(before * hot0, axis=0, keepdims=True).astype(jnp.int32)
        slot1 = jnp.sum(before * hot1, axis=0, keepdims=True).astype(jnp.int32)
        dest0 = id0 * capacity + slot0
        dest1 = id1 * capacity + slot1
        dest_ref[0:1, :] = dest0
        dest_ref[1:2, :] = dest1
        place = lax.broadcasted_iota(jnp.int32, (slots, tokens), 0)
        spread = jnp.where(place == dest0, weight_ref[0:1, :], 0.0) + jnp.where(
            place == dest1, weight_ref[1:2, :], 0.0
        )
        high = spread.astype(bf16)
        low = (spread - high.astype(f32)).astype(bf16)
        cot = cot_ref[...]
        to_chunks(dot(high, cot, 1, 0) + dot(low, cot, 1, 0), scratch)
        out_ref[...] = scratch[...].astype(bf16)

    return body


def pick_body(dest_ref, pick_ref):
    tokens, slots = pick_ref.shape
    row = lax.broadcasted_iota(jnp.int32, (tokens, tokens), 0)
    col = lax.broadcasted_iota(jnp.int32, (tokens, tokens), 1)
    dest0, dest1 = (
        jnp.sum(jnp.where(row == col, dest_ref[k : k + 1, :].astype(f32), 0.0), axis=1, keepdims=True)
        .astype(jnp.int32)
        for k in range(2)
    )
    place = lax.broadcasted_iota(jnp.int32, (tokens, slots), 1)
    pick_ref[...] = ((place == dest0) | (place == dest1)).astype(f32).astype(bf16)


def factors_body(rows_ref, gate_ref, up_ref, act_ref, for_up_ref, for_gate_ref):
    block = rows_ref.shape[0] // 3

    def step(i, _):
        at = pl.ds(pl.multiple_of(i * block, block), block)
        rows = rows_ref[at, :]
        gate_lin = dot(rows, gate_ref[...], 1, 0)
        up_lin = dot(rows, up_ref[...], 1, 0)
        gate_c = jnp.minimum(gate_lin, clamp_limit)
        up_c = jnp.clip(up_lin, -clamp_limit, clamp_limit)
        sigma = jax.nn.sigmoid(swish_alpha * gate_c)
        swish = gate_c * sigma
        act_ref[at, :] = ((up_c + 1.0) * swish).astype(bf16)
        up_open = (up_lin > -clamp_limit) & (up_lin < clamp_limit)
        for_up_ref[at, :] = jnp.where(up_open, swish, 0.0).astype(bf16)
        slope = (up_c + 1.0) * (sigma + swish_alpha * swish * (1.0 - sigma))
        for_gate_ref[at, :] = jnp.where(gate_lin < clamp_limit, slope, 0.0).astype(bf16)
        return 0

    lax.fori_loop(0, 3, step, 0)


def partial_far_body(chunks_ref, far_ref, rows_ref, far_top, far_bot, scratch):
    n, width = rows_ref.shape
    half = n // 2
    rows = from_chunks(chunks_ref[...], scratch, n, width // LANES)
    rows_ref[...] = rows
    value = dot(rows, far_ref[...], 1, 1).astype(bf16)
    far_top[...] = value[:half]
    far_bot[...] = value[half:]


def partial_rest_body(rows_ref, next_ref, prev_ref, own_ref, *outs):
    next_top, next_bot, prev_top, prev_bot, own_out, rows_out = outs
    rows = rows_ref[...]
    half = rows.shape[0] // 2
    rows_out[...] = rows
    for weight, top, bot in ((next_ref, next_top, next_bot), (prev_ref, prev_top, prev_bot)):
        value = dot(rows, weight[...], 1, 1).astype(bf16)
        top[...] = value[:half]
        bot[...] = value[half:]
    own_out[...] = dot(rows, own_ref[...], 1, 1).astype(bf16)


def block_of(ref, index, size):
    return ref[pl.ds(pl.multiple_of(index * size, size), size), :]


def hidden_grad_body(
    at_ref, own_ref, prev_top, near_top, next_bot, near_bot, up_ref, gate_ref, wg_ref, wu_ref,
    d_gate_ref, d_up_ref, far_top, far_bot,
):
    half = prev_top.shape[0]
    size = far_top.shape[1]
    count = wg_ref.shape[0] // size
    own = own_ref[...].astype(f32)
    top = own[:half] + prev_top[...].astype(f32) + near_top[...].astype(f32)
    bot = own[half:] + next_bot[...].astype(f32) + near_bot[...].astype(f32)
    d_act = jnp.concatenate([top, bot], axis=0)
    d_gate = (d_act * gate_ref[...].astype(f32)).astype(bf16)
    d_up = (d_act * up_ref[...].astype(f32)).astype(bf16)
    d_gate_ref[...] = d_gate
    d_up_ref[...] = d_up
    far = lax.rem(at_ref[0] + 2, count)
    value = dot(d_gate, block_of(wg_ref, far, size), 1, 1) + dot(d_up, block_of(wu_ref, far, size), 1, 1)
    value = value.astype(bf16)
    far_top[...] = value[:half]
    far_bot[...] = value[half:]


def input_grad_body(
    at_ref, d_gate_ref, d_up_ref, wg_ref, wu_ref, next_top, next_bot, prev_top, prev_bot, own_out
):
    half = next_top.shape[0]
    size = own_out.shape[1]
    count = wg_ref.shape[0] // size
    d_gate, d_up = d_gate_ref[...], d_up_ref[...]

    def part(shift):
        at = lax.rem(at_ref[0] + shift, count)
        value = dot(d_gate, block_of(wg_ref, at, size), 1, 1)
        value = value + dot(d_up, block_of(wu_ref, at, size), 1, 1)
        return value.astype(bf16)

    value = part(1)
    next_bot[...] = value[half:]
    next_top[...] = value[:half]
    value = part(count - 1)
    prev_top[...] = value[:half]
    prev_bot[...] = value[half:]
    own_out[...] = part(0)


def total_body(own_ref, prev_top, near_top, next_bot, near_bot, out_ref, scratch):
    half = prev_top.shape[0]
    own = own_ref[...].astype(f32)
    top = own[:half] + prev_top[...].astype(f32) + near_top[...].astype(f32)
    bot = own[half:] + next_bot[...].astype(f32) + near_bot[...].astype(f32)
    to_chunks(jnp.concatenate([top, bot], axis=0), scratch)
    out_ref[...] = scratch[...].astype(bf16)


def combine_body(chunks_ref, pick_ref, cot_ref, mix_ref, scratch):
    slots = pick_ref.shape[1]
    rows = from_chunks(chunks_ref[...], scratch, slots, cot_ref.shape[1] // LANES)
    mix = (cot_ref[...].astype(f32) + dot(pick_ref[...], rows, 1, 0)).astype(bf16)
    mix_ref[...] = mix


def down_near_body(at_ref, act_ref, *refs):
    *rows, out_ref = refs
    size = rows[0].shape[1]
    count = out_ref.shape[1] // size
    act = act_ref[...]
    for rows_ref, shift in zip(rows, (0, 1, count - 1)):
        at = lax.rem(at_ref[0] + shift, count)
        value = dot(act, rows_ref[...], 0, 0)
        out_ref[:, pl.ds(pl.multiple_of(at * size, size), size)] = value.astype(bf16)


def down_far_body(at_ref, act_ref, rows_ref, near_ref, *refs):
    *operands, out_ref, one, two, three, block, sem = refs
    for operand, copy in zip(operands, (one, two, three)):
        copy[...] = operand[...]
    size = rows_ref.shape[1]
    block[...] = dot(act_ref[...], rows_ref[...], 0, 0).astype(bf16)
    at = lax.rem(at_ref[0] + 2, out_ref.shape[1] // size)
    put = pltpu.make_async_copy(
        block, out_ref.at[:, pl.ds(pl.multiple_of(at * size, size), size)], sem
    )
    put.start()
    put.wait()


def proj_grad_body(columns):
    def body(core_ref, act_ref, *refs):
        *mixes, send_ref, keep_ref = refs
        size = mixes[0].shape[1]
        rows = act_ref.shape[1] // 2
        block = rows // columns
        first = core_ref[0] == 0
        act = act_ref[...]
        for s, mix_ref in enumerate(mixes):
            value = dot(act, mix_ref[...], 0, 0).reshape(block // 8, columns, 2, 8, size)
            for x in range(columns):
                zero, one = (value[:, x, core].reshape(block, size) for core in range(2))
                at = (slice(x * block, (x + 1) * block), slice(s * size, (s + 1) * size))
                send_ref[at] = jnp.where(first, one, zero).astype(bf16)
                keep_ref[at] = jnp.where(first, zero, one).astype(bf16)

    return body


def pair_sum_body(at_ref, near_ref, near_in_ref, far_ref, far_in_ref, *outs):
    size = outs[0].shape[0]
    count = near_ref.shape[0] // size
    near = near_ref.shape[1]
    for out_ref, shift in zip(outs, (0, 1, count - 1, 2)):
        at = lax.rem(at_ref[0] + shift, count)

        def total(one_ref, two_ref):
            one, two = block_of(one_ref, at, size), block_of(two_ref, at, size)
            return (one.astype(f32) + two.astype(f32)).astype(bf16)

        out_ref[:, :near] = total(near_ref, near_in_ref)
        out_ref[:, near:] = total(far_ref, far_in_ref)


def four_sum_body(*refs):
    *terms, out_ref = refs
    out_ref[...] = sum(term[...].astype(f32) for term in terms).astype(bf16)


def proj_total_body(at_ref, terms_ref, out_ref):
    rows, width = out_ref.shape
    count = 4
    terms = terms_ref[...].astype(f32)
    total = jnp.sum(terms.reshape(terms.shape[0] // rows, rows, width), axis=0)
    size = width // count
    for s, shift in enumerate((0, 1, count - 1, 2)):
        at = lax.rem(at_ref[0] + shift, count)
        out_ref[:, pl.ds(pl.multiple_of(at * size, size), size)] = total[:, s * size : (s + 1) * size]


def split(value, pieces):
    terms = []
    for _ in range(pieces):
        terms.append(value.astype(bf16))
        value = value - terms[-1].astype(f32)
    return terms


def row_sums(first, second, out_ref):
    ones = jnp.ones((8, first.shape[1]), bf16)
    one = sum(dot(ones, term, 1, 1) for term in split(first, 3))
    two = sum(dot(ones, term, 1, 1) for term in split(second, 3))
    row = lax.broadcasted_iota(jnp.int32, out_ref.shape, 0)
    out_ref[...] = jnp.where(row == 0, one, jnp.where(row == 1, two, 0.0))


def along_rows(sums, index):
    row = lax.broadcasted_iota(jnp.int32, (8, LANES), 0)
    chosen = (row == index).astype(f32).astype(bf16)
    return sum(dot(term, chosen, 0, 0) for term in split(sums, 3))


def widened(value, lanes):
    return jnp.concatenate([value] * (lanes // LANES), axis=1)


def stats_body(conv_ref, out_ref):
    conv = conv_ref[...].astype(f32)
    row_sums(conv, conv * conv, out_ref)


def norm_body(channels):
    def body(own, one, two, three, conv_ref, gain_ref, *outs):
        sums = own[...] + one[...] + two[...] + three[...]
        width = conv_ref.shape[1]
        mean = along_rows(sums, 0) / channels
        var = along_rows(sums, 1) / channels - mean * mean
        rstd = lax.rsqrt(var + norm_epsilon)
        xhat = (conv_ref[...].astype(f32) - widened(mean, width)) * widened(rstd, width)
        gain = gain_ref[...]
        normed = xhat * gain
        sigma = jax.nn.sigmoid(normed)
        act_ref, xhat_ref, slope_ref, rstd_ref = outs
        act_ref[...] = (normed * sigma).astype(bf16)
        rstd_ref[...] = rstd
        xhat_ref[...] = xhat
        slope_ref[...] = sigma * (1.0 + normed * (1.0 - sigma)) * gain

    return body


def norm_grad_body(at_ref, own, following, previous, far, proj_ref, xhat_ref, slope_ref, dxh_ref, sums_ref):
    size = own.shape[1]
    count = proj_ref.shape[1] // size
    value = None
    for shift, mix_ref in ((0, own), (1, following), (count - 1, previous), (2, far)):
        at = lax.rem(at_ref[0] + shift, count)
        weight = proj_ref[:, pl.ds(pl.multiple_of(at * size, size), size)]
        term = dot(mix_ref[...], weight, 1, 1)
        value = term if value is None else value + term
    dxh = value * slope_ref[...]
    dxh_ref[...] = dxh
    row_sums(dxh, dxh * xhat_ref[...], sums_ref)


def conv_grad_body(channels):
    def body(own, one, two, three, dxh_ref, xhat_ref, rstd_ref, out_ref, edge_ref):
        sums = own[...] + one[...] + two[...] + three[...]
        width = dxh_ref.shape[1]
        first = widened(along_rows(sums, 0) / channels, width)
        second = widened(along_rows(sums, 1) / channels, width)
        value = widened(rstd_ref[...], width) * (dxh_ref[...] - first - xhat_ref[...] * second)
        out_ref[...] = value
        edge_ref[...] = value[: edge_ref.shape[0]]

    return body


def conv_body(grad_ref, edge_ref, taps_ref, value_ref, gate_ref, value_out, gate_out, extended, moved):
    tokens, width = grad_ref.shape
    reach = taps_ref.shape[0]
    extended[:tokens, :] = grad_ref[...]
    extended[tokens:, :] = edge_ref[...]
    rows = moved.shape[1]
    block = 64

    def step(i, _):
        lanes = pl.ds(pl.multiple_of(i * LANES, LANES), LANES)
        for r in range(8):
            moved[r] = extended[r : r + rows, lanes]
        for start in range(0, tokens, block):
            total = jnp.zeros((block, LANES), f32)
            for offset in range(reach):
                tap = taps_ref[reach - 1 - offset : reach - offset, lanes]
                begin = start + offset // 8 * 8
                total = total + tap * moved[offset % 8, begin : begin + block, :]
            at = slice(start, start + block)
            sigma = jax.nn.sigmoid(gate_ref[at, lanes].astype(f32))
            scaled = total * sigma
            value_out[at, lanes] = scaled.astype(bf16)
            gate = scaled * value_ref[at, lanes].astype(f32) * (1.0 - sigma)
            gate_out[at, lanes] = gate.astype(bf16)
        return 0

    lax.fori_loop(0, width // LANES, step, 0)


def weight_grad_body(rows_ref, gate_ref, up_ref, gate_out, up_out):
    size = gate_ref.shape[1]
    both = jnp.concatenate([gate_ref[...], up_ref[...]], axis=1)

    def step(i, _):
        at = pl.ds(pl.multiple_of(i * size, size), size)
        value = dot(rows_ref[:, at], both, 0, 0)
        gate_out[at, :] = value[:, :size].astype(bf16)
        up_out[at, :] = value[:, size:].astype(bf16)
        return 0

    lax.fori_loop(0, rows_ref.shape[1] // size, step, 0)


def near_body(one_ref, two_ref, out_ref):
    out_ref[...] = (one_ref[...].astype(f32) + two_ref[...].astype(f32)).astype(bf16)


def near_sum(one, two):
    (value,) = kernel(near_body, (struct(one.shape),), one, two, flops=one.size, limit=4)
    return value


def exchanged(value):
    return shifted(value, TP, 1), shifted(value, TP, -1), shifted(value, TP, 2)


def reduce_over_ring(far_top, far_bot, rest):
    far_top_in = shifted(far_top, TP, 1)
    far_bot_in = shifted(far_bot, TP, -1)
    next_top, next_bot, prev_top, prev_bot, own = rest
    next_bot_in = shifted(next_bot, TP, 1)
    prev_top_in = shifted(prev_top, TP, -1)
    near_top = near_sum(next_top, far_top_in)
    near_bot = near_sum(prev_bot, far_bot_in)
    near_top_in = shifted(near_top, TP, 1)
    near_bot_in = shifted(near_bot, TP, -1)
    return own, prev_top_in, near_top_in, next_bot_in, near_bot_in


def per_device(
    cot_out,
    route_ids,
    route_weight,
    expert_inputs,
    w_gate,
    w_up,
    w_down,
    w_proj,
    conv_out,
    channel_norm_gain,
    taps,
    value_pre,
    gate_pre,
):
    experts = lax.axis_size(SP)
    ways = lax.axis_size(TP)
    tok_rows = cot_out.shape[0]
    slot_rows = expert_inputs.shape[1]
    capacity = slot_rows // experts
    local_cols = cot_out.shape[1]
    hidden = w_down.shape[1]
    half = slot_rows // 2
    parts = local_cols // LANES
    chunk_rows = slot_rows * parts
    at = lax.axis_index(TP)
    at_ref = at.reshape(1).astype(jnp.int32)
    core_ref = lax.axis_index(CORE).reshape(1).astype(jnp.int32)
    rows_in, gate_weight, up_weight, down_weight = expert_inputs[0], w_gate[0], w_up[0], w_down[0]
    chunk_scratch = pltpu.VMEM((chunk_rows, LANES), f32)

    outgoing, dest = kernel(
        dispatch_body(experts, capacity),
        (struct((chunk_rows, LANES)), struct((2, tok_rows), jnp.int32)),
        route_ids.T, route_weight.T, cot_out,
        flops=4 * tok_rows * slot_rows * local_cols, scratch=(chunk_scratch,),
        staged=(), to_hbm=(1,),
    )
    moved = lax.all_to_all(
        outgoing.reshape(experts, chunk_rows // experts, LANES), SP, 0, 0, tiled=True
    )
    dest, conv_late, down_late, rows_late, gate_late, up_late, _ = lax.optimization_barrier(
        (dest, conv_out, down_weight, rows_in, gate_weight, up_weight, outgoing)
    )

    def down_block(shift):
        start = (at + shift) % ways * local_cols
        return lax.dynamic_slice_in_dim(down_late, start, local_cols, 1)

    down_own = down_block(0)
    down_next = shifted(down_block(ways - 1), TP, -1)
    down_prev = shifted(down_block(1), TP, 1)
    down_far = shifted(down_block(2), TP, 2)
    act, for_up, for_gate = kernel(
        factors_body,
        (struct((slot_rows, hidden)),) * 3,
        rows_late, gate_late, up_late,
        flops=4 * slot_rows * hidden * local_cols * ways, staged=(),
    )
    (pick,) = kernel(
        pick_body, (struct((tok_rows, slot_rows)),), dest, flops=tok_rows * slot_rows * 8
    )
    channel_total = local_cols * ways
    tokens_8 = struct((8, tok_rows), f32)
    block = struct((tok_rows, local_cols), f32)
    (stats,) = kernel(stats_body, (tokens_8,), conv_late, flops=48 * tok_rows * local_cols, limit=8)
    stats_in = exchanged(stats)
    gain = channel_norm_gain.reshape(1, local_cols)
    moved, act, for_up, for_gate, pick, stats_in = lax.optimization_barrier(
        (moved, act, for_up, for_gate, pick, stats_in)
    )

    rows_near, far_top, far_bot = kernel(
        partial_far_body,
        (struct((slot_rows, local_cols)),) + (struct((half, hidden)),) * 2,
        moved.reshape(chunk_rows, LANES), down_far,
        flops=2 * slot_rows * local_cols * hidden, scratch=(chunk_scratch,),
    )
    *rest, rows_cot = kernel(
        partial_rest_body,
        (struct((half, hidden)),) * 4
        + (struct((slot_rows, hidden)), struct((slot_rows, local_cols))),
        rows_near, down_next, down_prev, down_own,
        flops=6 * slot_rows * local_cols * hidden, to_hbm=(5,),
    )
    act_terms = reduce_over_ring(far_top, far_bot, rest)
    d_gate, d_up, far_top, far_bot = kernel(
        hidden_grad_body,
        (struct((slot_rows, hidden)),) * 2 + (struct((half, local_cols)),) * 2,
        at_ref, *act_terms, for_up, for_gate, gate_weight, up_weight,
        flops=4 * slot_rows * local_cols * hidden, smem=1,
    )
    rest = kernel(
        input_grad_body,
        (struct((half, local_cols)),) * 4 + (struct((slot_rows, local_cols)),),
        at_ref, d_gate, d_up, gate_weight, up_weight,
        flops=12 * slot_rows * local_cols * hidden, smem=1,
    )
    grad_terms = reduce_over_ring(far_top, far_bot, rest)
    (returning,) = kernel(
        total_body,
        (struct((chunk_rows, LANES)),),
        *grad_terms,
        flops=slot_rows * local_cols * 8, scratch=(chunk_scratch,),
    )
    coming = lax.all_to_all(
        returning.reshape(experts, chunk_rows // experts, LANES), SP, 0, 0, tiled=True
    )
    grad_gate_part, grad_up_part = kernel(
        weight_grad_body,
        (struct((local_cols * ways, hidden)),) * 2,
        rows_in, d_gate, d_up,
        flops=4 * slot_rows * hidden * local_cols * ways, to_hbm=(0, 1),
    )
    rows_cot, _ = lax.optimization_barrier((rows_cot, returning))
    rows_prev = shifted(rows_cot, TP, 1)
    rows_next = shifted(rows_cot, TP, -1)
    coming, grad_gate_part, grad_up_part = lax.optimization_barrier(
        (coming, grad_gate_part, grad_up_part)
    )
    (mix,) = kernel(
        combine_body,
        (struct((tok_rows, local_cols)),),
        coming.reshape(chunk_rows, LANES), pick, cot_out,
        flops=2 * tok_rows * slot_rows * local_cols, scratch=(chunk_scratch,),
    )
    mix_far = shifted(mix, TP, 2)
    mix_prev = shifted(mix, TP, 1)
    mix_next = shifted(mix, TP, -1)
    conv_mid, _ = lax.optimization_barrier((conv_out, mix))
    act_conv, xhat, slope, rstd = kernel(
        norm_body(channel_total),
        (struct((tok_rows, local_cols)), block, block, struct((tok_rows, LANES), f32)),
        stats, *stats_in, conv_mid, gain,
        flops=20 * tok_rows * local_cols, limit=8, staged=(),
    )
    columns, planes = lax.axis_size(COLUMN), lax.axis_size(PLANE)
    width = local_cols * ways
    core_rows = local_cols // 2
    column_rows = core_rows // columns

    def proj_terms(mixes):
        return kernel(
            proj_grad_body(columns),
            (struct((core_rows, local_cols * len(mixes))),) * 2,
            core_ref, act_conv, *mixes,
            flops=2 * len(mixes) * tok_rows * local_cols * local_cols, smem=1,
            to_hbm=(1,),
        )

    send, keep = proj_terms((mix, mix_next, mix_prev))
    came = shifted(send, CORE, 1)
    send_far, keep_far = proj_terms((mix_far,))
    came_far = shifted(send_far, CORE, 1)
    pair_own, pair_next, pair_prev, pair_far = kernel(
        pair_sum_body,
        (struct((column_rows, width)),) * 4,
        lax.axis_index(COLUMN).reshape(1).astype(jnp.int32), keep, came, keep_far, came_far,
        flops=core_rows * width, smem=1, limit=8, staged=(1, 3),
    )
    far_pair = shifted(pair_far, COLUMN, 2)
    near_pairs = (shifted(pair_next, COLUMN, 1), shifted(pair_prev, COLUMN, -1))
    (column_sum,) = kernel(
        four_sum_body,
        (struct((column_rows, width)),),
        pair_own, far_pair, *near_pairs,
        flops=column_rows * width * 4, limit=8,
    )
    terms = lax.all_to_all(
        column_sum.reshape(planes, column_rows // planes, width), PLANE, 0, 0, tiled=True
    )
    (grad_proj,) = kernel(
        proj_total_body,
        (struct((column_rows // planes, width), f32),),
        at_ref, terms.reshape(column_rows, width),
        flops=column_rows * width, smem=1, limit=8, to_hbm=(0,),
    )
    dxh, sums = kernel(
        norm_grad_body,
        (block, tokens_8),
        at_ref, mix, mix_next, mix_prev, mix_far, w_proj, xhat, slope,
        flops=2 * tok_rows * local_cols * local_cols * ways, smem=1,
        staged=(0, 1, 2, 3, 5, 6),
    )
    sums_in = exchanged(sums)
    rows_far = shifted(rows_cot, TP, 2)
    (grad_down,) = kernel(
        down_near_body,
        (struct((hidden, width)),),
        at_ref, act, rows_cot, rows_next, rows_prev,
        flops=6 * slot_rows * hidden * local_cols, smem=1, to_hbm=(0,), staged=(),
    )
    hbm = pl.BlockSpec(memory_space=pltpu.HBM)
    vmem = pl.BlockSpec(memory_space=pltpu.VMEM)
    conv_operands = (taps, value_pre, gate_pre)
    grad_down, *conv_operands = pl.pallas_call(
        down_far_body,
        out_shape=(struct((hidden, width)),)
        + tuple(pltpu.VMEM(v.shape, v.dtype) for v in conv_operands),
        in_specs=[pl.BlockSpec(memory_space=pltpu.SMEM), vmem, vmem, hbm, vmem, vmem, vmem],
        out_specs=(hbm, vmem, vmem, vmem),
        scratch_shapes=[pltpu.VMEM((hidden, local_cols), bf16), pltpu.SemaphoreType.DMA],
        input_output_aliases={3: 0},
        cost_estimate=pl.CostEstimate(
            flops=2 * slot_rows * hidden * local_cols, transcendentals=0, bytes_accessed=1 << 20
        ),
        compiler_params=pltpu.CompilerParams(vmem_limit_bytes=24 << 20),
        name="down_far",
    )(
        at_ref,
        *(pltpu.with_memory_space_constraint(v, pltpu.HBM) for v in (act, rows_far, grad_down, *conv_operands)),
    )
    reach = taps.shape[0]
    convolution_gradient, edge = kernel(
        conv_grad_body(channel_total),
        (block, struct((32, local_cols), f32)),
        sums, *sums_in, dxh, xhat, rstd,
        flops=8 * tok_rows * local_cols, limit=8,
    )
    following = passed_along(edge, SP, -1)
    following, grad_down = lax.optimization_barrier((following, grad_down))
    grad_value, grad_gate = kernel(
        conv_body,
        (struct((tok_rows, local_cols)),) * 2,
        convolution_gradient, following, *conv_operands,
        flops=2 * reach * tok_rows * local_cols, limit=8, to_hbm=(0, 1),
        scratch=(
            pltpu.VMEM((tok_rows + edge.shape[0], local_cols), f32),
            pltpu.VMEM((8, tok_rows + 24, LANES), f32),
        ),
    )
    return (
        grad_gate_part[None],
        grad_up_part[None],
        grad_down[None],
        grad_proj,
        grad_value,
        grad_gate,
    )


def solution(mesh):
    finer = Mesh(mesh.devices.reshape(8, 4, 2, mesh.shape["tp"]), ("sp_0", "sp_1", "sp_2", "tp"))
    placed = (
        P(SP, "tp"),
        P(SP, None),
        P(SP, None),
        P(SP, None, None),
        P(SP, None, "tp"),
        P(SP, None, "tp"),
        P(SP, "tp", None),
        P("tp", None),
        P(SP, "tp"),
        P("tp"),
        P(None, "tp"),
        P(SP, "tp"),
        P(SP, "tp"),
    )

    return jax.shard_map(
        per_device,
        mesh=finer,
        in_specs=placed,
        out_specs=(
            P(SP, None, "tp"),
            P(SP, None, "tp"),
            P(SP, "tp", None),
            P(TP_SP, None),
            P(SP, "tp"),
            P(SP, "tp"),
        ),
        check_vma=False,
    )
```

```python
import jax
import jax.numpy as jnp
from jax import lax
from jax.experimental import pallas as pl
from jax.experimental.pallas import tpu as pltpu
from jax.sharding import Mesh
from jax.sharding import PartitionSpec as P

SP = ("sp_0", "sp_1", "sp_2")
PLANE = "sp_0"
COLUMN = "sp_1"
CORE = "sp_2"
TP = "tp"
TP_SP = ("tp", "sp_0", "sp_1", "sp_2")

clamp_limit = 7.0
swish_alpha = 1.702
norm_epsilon = 1e-05
LANES = 128
bf16 = jnp.bfloat16
f32 = jnp.float32


def shifted(value, axis, steps):
    count = lax.axis_size(axis)
    return lax.ppermute(value, axis, [(i, (i + steps) % count) for i in range(count)])


def passed_along(value, axis, steps):
    count = lax.axis_size(axis)
    leading, last = (max(0, -steps), min(count, count - steps))
    return lax.ppermute(value, axis, [(source, source + steps) for source in range(leading, last)])


def dot(a, b, ca, cb):
    return lax.dot_general(a, b, (((ca,), (cb,)), ((), ())), preferred_element_type=f32)


def kernel(body, outs, *args, flops, scratch=(), smem=0, limit=24, staged=range(99), to_hbm=()):
    spaces = [pltpu.SMEM] * smem + [pltpu.VMEM] * (len(args) - smem)
    moved = sum(a.size * a.dtype.itemsize for a in (*args[smem:], *outs))
    args = args[:smem] + tuple(
        pltpu.with_memory_space_constraint(a, pltpu.VMEM if i in staged else pltpu.HBM)
        for i, a in enumerate(args[smem:])
    )
    return pl.pallas_call(
        body,
        out_shape=tuple(
            (pltpu.HBM if i in to_hbm else pltpu.VMEM)(o.shape, o.dtype) for i, o in enumerate(outs)
        ),
        in_specs=[pl.BlockSpec(memory_space=s) for s in spaces],
        out_specs=tuple(pl.BlockSpec(memory_space=pltpu.VMEM) for _ in outs),
        scratch_shapes=list(scratch),
        cost_estimate=pl.CostEstimate(flops=flops, transcendentals=0, bytes_accessed=moved),
        compiler_params=pltpu.CompilerParams(vmem_limit_bytes=limit << 20),
    )(*args)


def struct(shape, dtype=bf16):
    return jax.ShapeDtypeStruct(shape, dtype)


def to_chunks(rows, scratch):
    n, parts = rows.shape[0], rows.shape[1] // LANES
    for j in range(parts):
        scratch[pl.ds(j, n, stride=parts), :] = rows[:, j * LANES : (j + 1) * LANES]


def from_chunks(chunks, scratch, n, parts):
    scratch[...] = chunks.astype(f32)
    pieces = [scratch[pl.ds(j, n, stride=parts), :].astype(bf16) for j in range(parts)]
    return jnp.concatenate(pieces, axis=1)


def dispatch_body(experts, capacity):
    def body(ids_ref, weight_ref, cot_ref, out_ref, dest_ref, scratch):
        tokens = ids_ref.shape[1]
        slots = experts * capacity
        id0, id1 = ids_ref[0:1, :], ids_ref[1:2, :]
        expert = lax.broadcasted_iota(jnp.int32, (LANES, tokens), 0)
        hot0 = (id0 == expert).astype(f32)
        hot1 = (id1 == expert).astype(f32)
        row = lax.broadcasted_iota(jnp.int32, (tokens, tokens), 0)
        col = lax.broadcasted_iota(jnp.int32, (tokens, tokens), 1)
        before = dot((hot0 + hot1).astype(bf16), (row < col).astype(f32).astype(bf16), 1, 0)
        slot0 = jnp.sum(before * hot0, axis=0, keepdims=True).astype(jnp.int32)
        slot1 = jnp.sum(before * hot1, axis=0, keepdims=True).astype(jnp.int32)
        dest0 = id0 * capacity + slot0
        dest1 = id1 * capacity + slot1
        dest_ref[0:1, :] = dest0
        dest_ref[1:2, :] = dest1
        place = lax.broadcasted_iota(jnp.int32, (slots, tokens), 0)
        spread = jnp.where(place == dest0, weight_ref[0:1, :], 0.0) + jnp.where(
            place == dest1, weight_ref[1:2, :], 0.0
        )
        high = spread.astype(bf16)
        low = (spread - high.astype(f32)).astype(bf16)
        cot = cot_ref[...]
        to_chunks(dot(high, cot, 1, 0) + dot(low, cot, 1, 0), scratch)
        out_ref[...] = scratch[...].astype(bf16)

    return body


def pick_body(dest_ref, pick_ref):
    tokens, slots = pick_ref.shape
    row = lax.broadcasted_iota(jnp.int32, (tokens, tokens), 0)
    col = lax.broadcasted_iota(jnp.int32, (tokens, tokens), 1)
    dest0, dest1 = (
        jnp.sum(jnp.where(row == col, dest_ref[k : k + 1, :].astype(f32), 0.0), axis=1, keepdims=True)
        .astype(jnp.int32)
        for k in range(2)
    )
    place = lax.broadcasted_iota(jnp.int32, (tokens, slots), 1)
    pick_ref[...] = ((place == dest0) | (place == dest1)).astype(f32).astype(bf16)


def factors_body(rows_ref, gate_ref, up_ref, act_ref, for_up_ref, for_gate_ref):
    block = rows_ref.shape[0] // 3

    def step(i, _):
        at = pl.ds(pl.multiple_of(i * block, block), block)
        rows = rows_ref[at, :]
        gate_lin = dot(rows, gate_ref[...], 1, 0)
        up_lin = dot(rows, up_ref[...], 1, 0)
        gate_c = jnp.minimum(gate_lin, clamp_limit)
        up_c = jnp.clip(up_lin, -clamp_limit, clamp_limit)
        sigma = jax.nn.sigmoid(swish_alpha * gate_c)
        swish = gate_c * sigma
        act_ref[at, :] = ((up_c + 1.0) * swish).astype(bf16)
        up_open = (up_lin > -clamp_limit) & (up_lin < clamp_limit)
        for_up_ref[at, :] = jnp.where(up_open, swish, 0.0).astype(bf16)
        slope = (up_c + 1.0) * (sigma + swish_alpha * swish * (1.0 - sigma))
        for_gate_ref[at, :] = jnp.where(gate_lin < clamp_limit, slope, 0.0).astype(bf16)
        return 0

    lax.fori_loop(0, 3, step, 0)


def partial_act_body(chunks_ref, far_ref, next_ref, prev_ref, own_ref, *outs_scratch):
    rows_ref, far_top, far_bot, next_top, next_bot, prev_top, prev_bot, own_out, scratch = outs_scratch
    n, width = rows_ref.shape
    half = n // 2
    rows = from_chunks(chunks_ref[...], scratch, n, width // LANES)
    rows_ref[...] = rows
    for weight, top, bot in (
        (far_ref, far_top, far_bot),
        (next_ref, next_top, next_bot),
        (prev_ref, prev_top, prev_bot),
    ):
        value = dot(rows, weight[...], 1, 1).astype(bf16)
        top[...] = value[:half]
        bot[...] = value[half:]
    own_out[...] = dot(rows, own_ref[...], 1, 1).astype(bf16)


def block_of(ref, index, size):
    return ref[pl.ds(pl.multiple_of(index * size, size), size), :]


def hidden_grad_body(
    at_ref, own_ref, prev_top, near_top, next_bot, near_bot, up_ref, gate_ref, wg_ref, wu_ref,
    d_gate_ref, d_up_ref, far_top, far_bot,
):
    half = prev_top.shape[0]
    size = far_top.shape[1]
    count = wg_ref.shape[0] // size
    own = own_ref[...].astype(f32)
    top = own[:half] + prev_top[...].astype(f32) + near_top[...].astype(f32)
    bot = own[half:] + next_bot[...].astype(f32) + near_bot[...].astype(f32)
    d_act = jnp.concatenate([top, bot], axis=0)
    d_gate = (d_act * gate_ref[...].astype(f32)).astype(bf16)
    d_up = (d_act * up_ref[...].astype(f32)).astype(bf16)
    d_gate_ref[...] = d_gate
    d_up_ref[...] = d_up
    far = lax.rem(at_ref[0] + 2, count)
    value = dot(d_gate, block_of(wg_ref, far, size), 1, 1) + dot(d_up, block_of(wu_ref, far, size), 1, 1)
    value = value.astype(bf16)
    far_top[...] = value[:half]
    far_bot[...] = value[half:]


def input_grad_body(
    at_ref, d_gate_ref, d_up_ref, wg_ref, wu_ref, next_top, next_bot, prev_top, prev_bot, own_out
):
    half = next_top.shape[0]
    size = own_out.shape[1]
    count = wg_ref.shape[0] // size
    d_gate, d_up = d_gate_ref[...], d_up_ref[...]

    def part(shift):
        at = lax.rem(at_ref[0] + shift, count)
        value = dot(d_gate, block_of(wg_ref, at, size), 1, 1)
        value = value + dot(d_up, block_of(wu_ref, at, size), 1, 1)
        return value.astype(bf16)

    value = part(1)
    next_bot[...] = value[half:]
    next_top[...] = value[:half]
    value = part(count - 1)
    prev_top[...] = value[:half]
    prev_bot[...] = value[half:]
    own_out[...] = part(0)


def total_body(own_ref, prev_top, near_top, next_bot, near_bot, out_ref, scratch):
    half = prev_top.shape[0]
    own = own_ref[...].astype(f32)
    top = own[:half] + prev_top[...].astype(f32) + near_top[...].astype(f32)
    bot = own[half:] + next_bot[...].astype(f32) + near_bot[...].astype(f32)
    to_chunks(jnp.concatenate([top, bot], axis=0), scratch)
    out_ref[...] = scratch[...].astype(bf16)


def combine_body(chunks_ref, pick_ref, cot_ref, mix_ref, scratch):
    slots = pick_ref.shape[1]
    rows = from_chunks(chunks_ref[...], scratch, slots, cot_ref.shape[1] // LANES)
    mix = (cot_ref[...].astype(f32) + dot(pick_ref[...], rows, 1, 0)).astype(bf16)
    mix_ref[...] = mix


def down_near_body(at_ref, act_ref, *refs):
    *rows, out_ref = refs
    size = rows[0].shape[1]
    count = out_ref.shape[1] // size
    act = act_ref[...]
    for rows_ref, shift in zip(rows, (0, 1, count - 1)):
        at = lax.rem(at_ref[0] + shift, count)
        value = dot(act, rows_ref[...], 0, 0)
        out_ref[:, pl.ds(pl.multiple_of(at * size, size), size)] = value.astype(bf16)


def down_far_body(at_ref, act_ref, rows_ref, near_ref, out_ref, block, sem):
    size = rows_ref.shape[1]
    block[...] = dot(act_ref[...], rows_ref[...], 0, 0).astype(bf16)
    at = lax.rem(at_ref[0] + 2, out_ref.shape[1] // size)
    put = pltpu.make_async_copy(
        block, out_ref.at[:, pl.ds(pl.multiple_of(at * size, size), size)], sem
    )
    put.start()
    put.wait()


def proj_grad_body(columns):
    def body(core_ref, act_ref, *refs):
        *mixes, send_ref, keep_ref = refs
        size = mixes[0].shape[1]
        rows = act_ref.shape[1] // 2
        block = rows // columns
        first = core_ref[0] == 0
        act = act_ref[...]
        for s, mix_ref in enumerate(mixes):
            value = dot(act, mix_ref[...], 0, 0).reshape(block // 8, columns, 2, 8, size)
            at = slice(s * size, (s + 1) * size)

            def store(core, out_ref, value=value, at=at):
                for x in range(columns):
                    half = value[:, x, core].reshape(block, size)
                    out_ref[x * block : (x + 1) * block, at] = half.astype(bf16)

            @pl.when(first)
            def _():
                store(1, send_ref)
                store(0, keep_ref)

            @pl.when(jnp.logical_not(first))
            def _():
                store(0, send_ref)
                store(1, keep_ref)

    return body


def pair_sum_body(at_ref, near_ref, near_in_ref, far_ref, far_in_ref, *outs):
    size = outs[0].shape[0]
    count = near_ref.shape[0] // size
    near = near_ref.shape[1]
    for out_ref, shift in zip(outs, (0, 1, count - 1, 2)):
        at = lax.rem(at_ref[0] + shift, count)

        def total(one_ref, two_ref):
            one, two = block_of(one_ref, at, size), block_of(two_ref, at, size)
            return (one.astype(f32) + two.astype(f32)).astype(bf16)

        out_ref[:, :near] = total(near_ref, near_in_ref)
        out_ref[:, near:] = total(far_ref, far_in_ref)


def four_sum_body(*refs):
    *terms, out_ref = refs
    out_ref[...] = sum(term[...].astype(f32) for term in terms).astype(bf16)


def proj_total_body(at_ref, terms_ref, out_ref):
    rows, width = out_ref.shape
    count = 4
    terms = terms_ref[...].astype(f32)
    total = jnp.sum(terms.reshape(terms.shape[0] // rows, rows, width), axis=0)
    size = width // count
    for s, shift in enumerate((0, 1, count - 1, 2)):
        at = lax.rem(at_ref[0] + shift, count)
        out_ref[:, pl.ds(pl.multiple_of(at * size, size), size)] = total[:, s * size : (s + 1) * size]


def split(value, pieces):
    terms = []
    for _ in range(pieces):
        terms.append(value.astype(bf16))
        value = value - terms[-1].astype(f32)
    return terms


def row_sums(first, second, out_ref):
    ones = jnp.ones((8, first.shape[1]), bf16)
    one = sum(dot(ones, term, 1, 1) for term in split(first, 3))
    two = sum(dot(ones, term, 1, 1) for term in split(second, 3))
    row = lax.broadcasted_iota(jnp.int32, out_ref.shape, 0)
    out_ref[...] = jnp.where(row == 0, one, jnp.where(row == 1, two, 0.0))


def along_rows(sums, index):
    row = lax.broadcasted_iota(jnp.int32, (8, LANES), 0)
    chosen = (row == index).astype(f32).astype(bf16)
    return sum(dot(term, chosen, 0, 0) for term in split(sums, 3))


def widened(value, lanes):
    return jnp.concatenate([value] * (lanes // LANES), axis=1)


def stats_body(conv_ref, out_ref):
    conv = conv_ref[...].astype(f32)
    row_sums(conv, conv * conv, out_ref)


def norm_body(channels):
    def body(own, one, two, three, conv_ref, gain_ref, *outs):
        sums = own[...] + one[...] + two[...] + three[...]
        width = conv_ref.shape[1]
        mean = along_rows(sums, 0) / channels
        var = along_rows(sums, 1) / channels - mean * mean
        rstd = lax.rsqrt(var + norm_epsilon)
        xhat = (conv_ref[...].astype(f32) - widened(mean, width)) * widened(rstd, width)
        gain = gain_ref[...]
        normed = xhat * gain
        sigma = jax.nn.sigmoid(normed)
        act_ref, xhat_ref, slope_ref, rstd_ref = outs
        act_ref[...] = (normed * sigma).astype(bf16)
        rstd_ref[...] = rstd
        xhat_ref[...] = xhat
        slope_ref[...] = sigma * (1.0 + normed * (1.0 - sigma)) * gain

    return body


def norm_grad_body(at_ref, own, following, previous, far, proj_ref, xhat_ref, slope_ref, dxh_ref, sums_ref):
    size = own.shape[1]
    count = proj_ref.shape[1] // size
    value = None
    for shift, mix_ref in ((0, own), (1, following), (count - 1, previous), (2, far)):
        at = lax.rem(at_ref[0] + shift, count)
        weight = proj_ref[:, pl.ds(pl.multiple_of(at * size, size), size)]
        term = dot(mix_ref[...], weight, 1, 1)
        value = term if value is None else value + term
    dxh = value * slope_ref[...]
    dxh_ref[...] = dxh
    row_sums(dxh, dxh * xhat_ref[...], sums_ref)


def conv_grad_body(channels):
    def body(own, one, two, three, dxh_ref, xhat_ref, rstd_ref, out_ref, edge_ref):
        sums = own[...] + one[...] + two[...] + three[...]
        width = dxh_ref.shape[1]
        first = widened(along_rows(sums, 0) / channels, width)
        second = widened(along_rows(sums, 1) / channels, width)
        value = widened(rstd_ref[...], width) * (dxh_ref[...] - first - xhat_ref[...] * second)
        out_ref[...] = value
        edge_ref[...] = value[: edge_ref.shape[0]]

    return body


def conv_body(grad_ref, edge_ref, taps_ref, value_ref, gate_ref, value_out, gate_out, extended, moved):
    tokens, width = grad_ref.shape
    reach = taps_ref.shape[0]
    extended[:tokens, :] = grad_ref[...]
    extended[tokens:, :] = edge_ref[...]
    rows = moved.shape[1]
    block = 64

    def step(i, _):
        lanes = pl.ds(pl.multiple_of(i * LANES, LANES), LANES)
        for r in range(8):
            moved[r] = extended[r : r + rows, lanes]
        for start in range(0, tokens, block):
            total = jnp.zeros((block, LANES), f32)
            for offset in range(reach):
                tap = taps_ref[reach - 1 - offset : reach - offset, lanes]
                begin = start + offset // 8 * 8
                total = total + tap * moved[offset % 8, begin : begin + block, :]
            at = slice(start, start + block)
            sigma = jax.nn.sigmoid(gate_ref[at, lanes].astype(f32))
            scaled = total * sigma
            value_out[at, lanes] = scaled.astype(bf16)
            gate = scaled * value_ref[at, lanes].astype(f32) * (1.0 - sigma)
            gate_out[at, lanes] = gate.astype(bf16)
        return 0

    lax.fori_loop(0, width // LANES, step, 0)


def weight_grad_body(rows_ref, gate_ref, up_ref, gate_out, up_out):
    size = gate_ref.shape[1]
    both = jnp.concatenate([gate_ref[...], up_ref[...]], axis=1)

    def step(i, _):
        at = pl.ds(pl.multiple_of(i * size, size), size)
        value = dot(rows_ref[:, at], both, 0, 0)
        gate_out[at, :] = value[:, :size].astype(bf16)
        up_out[at, :] = value[:, size:].astype(bf16)
        return 0

    lax.fori_loop(0, rows_ref.shape[1] // size, step, 0)


def near_body(one_ref, two_ref, out_ref):
    out_ref[...] = (one_ref[...].astype(f32) + two_ref[...].astype(f32)).astype(bf16)


def near_sum(one, two):
    (value,) = kernel(near_body, (struct(one.shape),), one, two, flops=one.size, limit=4)
    return value


def exchanged(value):
    return shifted(value, TP, 1), shifted(value, TP, -1), shifted(value, TP, 2)


def reduce_over_ring(far_top, far_bot, rest):
    far_top_in = shifted(far_top, TP, 1)
    far_bot_in = shifted(far_bot, TP, -1)
    next_top, next_bot, prev_top, prev_bot, own = rest
    next_bot_in = shifted(next_bot, TP, 1)
    prev_top_in = shifted(prev_top, TP, -1)
    near_top = near_sum(next_top, far_top_in)
    near_bot = near_sum(prev_bot, far_bot_in)
    near_top_in = shifted(near_top, TP, 1)
    near_bot_in = shifted(near_bot, TP, -1)
    return own, prev_top_in, near_top_in, next_bot_in, near_bot_in


def per_device(
    cot_out,
    route_ids,
    route_weight,
    expert_inputs,
    w_gate,
    w_up,
    w_down,
    w_proj,
    conv_out,
    channel_norm_gain,
    taps,
    value_pre,
    gate_pre,
):
    experts = lax.axis_size(SP)
    ways = lax.axis_size(TP)
    tok_rows = cot_out.shape[0]
    slot_rows = expert_inputs.shape[1]
    capacity = slot_rows // experts
    local_cols = cot_out.shape[1]
    hidden = w_down.shape[1]
    half = slot_rows // 2
    parts = local_cols // LANES
    chunk_rows = slot_rows * parts
    at = lax.axis_index(TP)
    at_ref = at.reshape(1).astype(jnp.int32)
    core_ref = lax.axis_index(CORE).reshape(1).astype(jnp.int32)
    rows_in, gate_weight, up_weight, down_weight = expert_inputs[0], w_gate[0], w_up[0], w_down[0]
    chunk_scratch = pltpu.VMEM((chunk_rows, LANES), f32)

    outgoing, dest = kernel(
        dispatch_body(experts, capacity),
        (struct((chunk_rows, LANES)), struct((2, tok_rows), jnp.int32)),
        route_ids.T, route_weight.T, cot_out,
        flops=4 * tok_rows * slot_rows * local_cols, scratch=(chunk_scratch,),
        staged=(), to_hbm=(0, 1),
    )
    moved = lax.all_to_all(
        outgoing.reshape(experts, chunk_rows // experts, LANES), SP, 0, 0, tiled=True
    )
    dest, conv_late, down_late, rows_late, gate_late, up_late = lax.optimization_barrier(
        (dest, conv_out, down_weight, rows_in, gate_weight, up_weight)
    )

    def down_block(shift):
        start = (at + shift) % ways * local_cols
        return lax.dynamic_slice_in_dim(down_late, start, local_cols, 1)

    down_own = down_block(0)
    down_next = shifted(down_block(ways - 1), TP, -1)
    down_prev = shifted(down_block(1), TP, 1)
    down_far = shifted(down_block(2), TP, 2)
    act, for_up, for_gate = kernel(
        factors_body,
        (struct((slot_rows, hidden)),) * 3,
        rows_late, gate_late, up_late,
        flops=4 * slot_rows * hidden * local_cols * ways,
    )
    (pick,) = kernel(
        pick_body, (struct((tok_rows, slot_rows)),), dest, flops=tok_rows * slot_rows * 8
    )
    channel_total = local_cols * ways
    tokens_8 = struct((8, tok_rows), f32)
    block = struct((tok_rows, local_cols), f32)
    (stats,) = kernel(stats_body, (tokens_8,), conv_late, flops=48 * tok_rows * local_cols, limit=8)
    stats_in = exchanged(stats)
    gain = channel_norm_gain.reshape(1, local_cols)
    moved, act, for_up, for_gate, pick, stats_in = lax.optimization_barrier(
        (moved, act, for_up, for_gate, pick, stats_in)
    )

    rows_cot, far_top, far_bot, *rest = kernel(
        partial_act_body,
        (struct((slot_rows, local_cols)),) + (struct((half, hidden)),) * 6
        + (struct((slot_rows, hidden)),),
        moved.reshape(chunk_rows, LANES), down_far, down_next, down_prev, down_own,
        flops=2 * slot_rows * local_cols * hidden * ways,
        scratch=(chunk_scratch,), to_hbm=(0,),
    )
    act_terms = reduce_over_ring(far_top, far_bot, rest)
    d_gate, d_up, far_top, far_bot = kernel(
        hidden_grad_body,
        (struct((slot_rows, hidden)),) * 2 + (struct((half, local_cols)),) * 2,
        at_ref, *act_terms, for_up, for_gate, gate_weight, up_weight,
        flops=4 * slot_rows * local_cols * hidden, smem=1,
    )
    rest = kernel(
        input_grad_body,
        (struct((half, local_cols)),) * 4 + (struct((slot_rows, local_cols)),),
        at_ref, d_gate, d_up, gate_weight, up_weight,
        flops=12 * slot_rows * local_cols * hidden, smem=1,
    )
    grad_terms = reduce_over_ring(far_top, far_bot, rest)
    (returning,) = kernel(
        total_body,
        (struct((chunk_rows, LANES)),),
        *grad_terms,
        flops=slot_rows * local_cols * 8, scratch=(chunk_scratch,),
    )
    coming = lax.all_to_all(
        returning.reshape(experts, chunk_rows // experts, LANES), SP, 0, 0, tiled=True
    )
    grad_gate_part, grad_up_part = kernel(
        weight_grad_body,
        (struct((local_cols * ways, hidden)),) * 2,
        rows_in, d_gate, d_up,
        flops=4 * slot_rows * hidden * local_cols * ways, to_hbm=(0, 1),
    )
    rows_cot, _ = lax.optimization_barrier((rows_cot, returning))
    rows_prev = shifted(rows_cot, TP, 1)
    rows_next = shifted(rows_cot, TP, -1)
    coming, grad_gate_part, grad_up_part = lax.optimization_barrier(
        (coming, grad_gate_part, grad_up_part)
    )
    (mix,) = kernel(
        combine_body,
        (struct((tok_rows, local_cols)),),
        coming.reshape(chunk_rows, LANES), pick, cot_out,
        flops=2 * tok_rows * slot_rows * local_cols, scratch=(chunk_scratch,),
    )
    mix_far = shifted(mix, TP, 2)
    mix_prev = shifted(mix, TP, 1)
    mix_next = shifted(mix, TP, -1)
    conv_mid, _ = lax.optimization_barrier((conv_out, mix))
    act_conv, xhat, slope, rstd = kernel(
        norm_body(channel_total),
        (struct((tok_rows, local_cols)), block, block, struct((tok_rows, LANES), f32)),
        stats, *stats_in, conv_mid, gain,
        flops=20 * tok_rows * local_cols, limit=8, staged=(),
    )
    columns, planes = lax.axis_size(COLUMN), lax.axis_size(PLANE)
    width = local_cols * ways
    core_rows = local_cols // 2
    column_rows = core_rows // columns

    def proj_terms(mixes):
        return kernel(
            proj_grad_body(columns),
            (struct((core_rows, local_cols * len(mixes))),) * 2,
            core_ref, act_conv, *mixes,
            flops=2 * len(mixes) * tok_rows * local_cols * local_cols, smem=1,
            to_hbm=(1,),
        )

    send, keep = proj_terms((mix, mix_next, mix_prev))
    came = shifted(send, CORE, 1)
    send_far, keep_far = proj_terms((mix_far,))
    came_far = shifted(send_far, CORE, 1)
    pair_own, pair_next, pair_prev, pair_far = kernel(
        pair_sum_body,
        (struct((column_rows, width)),) * 4,
        lax.axis_index(COLUMN).reshape(1).astype(jnp.int32), keep, came, keep_far, came_far,
        flops=core_rows * width, smem=1, limit=8, staged=(1, 3),
    )
    far_pair = shifted(pair_far, COLUMN, 2)
    near_pairs = (shifted(pair_next, COLUMN, 1), shifted(pair_prev, COLUMN, -1))
    (column_sum,) = kernel(
        four_sum_body,
        (struct((column_rows, width)),),
        pair_own, far_pair, *near_pairs,
        flops=column_rows * width * 4, limit=8,
    )
    terms = lax.all_to_all(
        column_sum.reshape(planes, column_rows // planes, width), PLANE, 0, 0, tiled=True
    )
    (grad_proj,) = kernel(
        proj_total_body,
        (struct((column_rows // planes, width), f32),),
        at_ref, terms.reshape(column_rows, width),
        flops=column_rows * width, smem=1, limit=8, to_hbm=(0,),
    )
    dxh, sums = kernel(
        norm_grad_body,
        (block, tokens_8),
        at_ref, mix, mix_next, mix_prev, mix_far, w_proj, xhat, slope,
        flops=2 * tok_rows * local_cols * local_cols * ways, smem=1,
        staged=(0, 1, 2, 3, 5, 6),
    )
    sums_in = exchanged(sums)
    rows_far = shifted(rows_cot, TP, 2)
    (grad_down,) = kernel(
        down_near_body,
        (struct((hidden, width)),),
        at_ref, act, rows_cot, rows_next, rows_prev,
        flops=6 * slot_rows * hidden * local_cols, smem=1, to_hbm=(0,), staged=(),
    )
    hbm = pl.BlockSpec(memory_space=pltpu.HBM)
    vmem = pl.BlockSpec(memory_space=pltpu.VMEM)
    grad_down = pl.pallas_call(
        down_far_body,
        out_shape=struct((hidden, width)),
        in_specs=[pl.BlockSpec(memory_space=pltpu.SMEM), vmem, vmem, hbm],
        out_specs=hbm,
        scratch_shapes=[pltpu.VMEM((hidden, local_cols), bf16), pltpu.SemaphoreType.DMA],
        input_output_aliases={3: 0},
        cost_estimate=pl.CostEstimate(
            flops=2 * slot_rows * hidden * local_cols, transcendentals=0, bytes_accessed=1 << 20
        ),
        compiler_params=pltpu.CompilerParams(vmem_limit_bytes=24 << 20),
        name="down_far",
    )(
        at_ref,
        *(pltpu.with_memory_space_constraint(v, pltpu.HBM) for v in (act, rows_far, grad_down)),
    )
    reach = taps.shape[0]
    convolution_gradient, edge = kernel(
        conv_grad_body(channel_total),
        (block, struct((32, local_cols), f32)),
        sums, *sums_in, dxh, xhat, rstd,
        flops=8 * tok_rows * local_cols, limit=8,
    )
    following = passed_along(edge, SP, -1)
    following, grad_down = lax.optimization_barrier((following, grad_down))
    grad_value, grad_gate = kernel(
        conv_body,
        (struct((tok_rows, local_cols)),) * 2,
        convolution_gradient, following, taps, value_pre, gate_pre,
        flops=2 * reach * tok_rows * local_cols, limit=8, to_hbm=(0, 1),
        staged=(0, 1),
        scratch=(
            pltpu.VMEM((tok_rows + edge.shape[0], local_cols), f32),
            pltpu.VMEM((8, tok_rows + 24, LANES), f32),
        ),
    )
    return (
        grad_gate_part[None],
        grad_up_part[None],
        grad_down[None],
        grad_proj,
        grad_value,
        grad_gate,
    )


def solution(mesh):
    finer = Mesh(mesh.devices.reshape(8, 4, 2, mesh.shape["tp"]), ("sp_0", "sp_1", "sp_2", "tp"))
    placed = (
        P(SP, "tp"),
        P(SP, None),
        P(SP, None),
        P(SP, None, None),
        P(SP, None, "tp"),
        P(SP, None, "tp"),
        P(SP, "tp", None),
        P("tp", None),
        P(SP, "tp"),
        P("tp"),
        P(None, "tp"),
        P(SP, "tp"),
        P(SP, "tp"),
    )

    return jax.shard_map(
        per_device,
        mesh=finer,
        in_specs=placed,
        out_specs=(
            P(SP, None, "tp"),
            P(SP, None, "tp"),
            P(SP, "tp", None),
            P(TP_SP, None),
            P(SP, "tp"),
            P(SP, "tp"),
        ),
        check_vma=False,
    )
```

```python
import jax
import jax.numpy as jnp
from jax import lax
from jax.experimental import pallas as pl
from jax.experimental.pallas import tpu as pltpu
from jax.sharding import Mesh
from jax.sharding import PartitionSpec as P

SP = ("sp_0", "sp_1", "sp_2")
PLANE = "sp_0"
COLUMN = "sp_1"
CORE = "sp_2"
TP = "tp"
TP_SP = ("tp", "sp_0", "sp_1", "sp_2")

clamp_limit = 7.0
swish_alpha = 1.702
norm_epsilon = 1e-05
LANES = 128
bf16 = jnp.bfloat16
f32 = jnp.float32


def shifted(value, axis, steps):
    count = lax.axis_size(axis)
    return lax.ppermute(value, axis, [(i, (i + steps) % count) for i in range(count)])


def passed_along(value, axis, steps):
    count = lax.axis_size(axis)
    leading, last = (max(0, -steps), min(count, count - steps))
    return lax.ppermute(value, axis, [(source, source + steps) for source in range(leading, last)])


def dot(a, b, ca, cb):
    return lax.dot_general(a, b, (((ca,), (cb,)), ((), ())), preferred_element_type=f32)


def kernel(body, outs, *args, flops, scratch=(), smem=0, limit=24, staged=range(99), to_hbm=()):
    spaces = [pltpu.SMEM] * smem + [pltpu.VMEM] * (len(args) - smem)
    moved = sum(a.size * a.dtype.itemsize for a in (*args[smem:], *outs))
    args = args[:smem] + tuple(
        pltpu.with_memory_space_constraint(a, pltpu.VMEM if i in staged else pltpu.HBM)
        for i, a in enumerate(args[smem:])
    )
    return pl.pallas_call(
        body,
        out_shape=tuple(
            (pltpu.HBM if i in to_hbm else pltpu.VMEM)(o.shape, o.dtype) for i, o in enumerate(outs)
        ),
        in_specs=[pl.BlockSpec(memory_space=s) for s in spaces],
        out_specs=tuple(pl.BlockSpec(memory_space=pltpu.VMEM) for _ in outs),
        scratch_shapes=list(scratch),
        cost_estimate=pl.CostEstimate(flops=flops, transcendentals=0, bytes_accessed=moved),
        compiler_params=pltpu.CompilerParams(vmem_limit_bytes=limit << 20),
    )(*args)


def struct(shape, dtype=bf16):
    return jax.ShapeDtypeStruct(shape, dtype)


def to_chunks(rows, scratch):
    n, parts = rows.shape[0], rows.shape[1] // LANES
    for j in range(parts):
        scratch[pl.ds(j, n, stride=parts), :] = rows[:, j * LANES : (j + 1) * LANES]


def from_chunks(chunks, scratch, n, parts):
    scratch[...] = chunks.astype(f32)
    pieces = [scratch[pl.ds(j, n, stride=parts), :].astype(bf16) for j in range(parts)]
    return jnp.concatenate(pieces, axis=1)


def dispatch_body(experts, capacity):
    def body(ids_ref, weight_ref, cot_ref, out_ref, dest_ref, scratch):
        tokens = ids_ref.shape[1]
        slots = experts * capacity
        id0, id1 = ids_ref[0:1, :], ids_ref[1:2, :]
        expert = lax.broadcasted_iota(jnp.int32, (LANES, tokens), 0)
        hot0 = (id0 == expert).astype(f32)
        hot1 = (id1 == expert).astype(f32)
        row = lax.broadcasted_iota(jnp.int32, (tokens, tokens), 0)
        col = lax.broadcasted_iota(jnp.int32, (tokens, tokens), 1)
        before = dot((hot0 + hot1).astype(bf16), (row < col).astype(f32).astype(bf16), 1, 0)
        slot0 = jnp.sum(before * hot0, axis=0, keepdims=True).astype(jnp.int32)
        slot1 = jnp.sum(before * hot1, axis=0, keepdims=True).astype(jnp.int32)
        dest0 = id0 * capacity + slot0
        dest1 = id1 * capacity + slot1
        dest_ref[0:1, :] = dest0
        dest_ref[1:2, :] = dest1
        place = lax.broadcasted_iota(jnp.int32, (slots, tokens), 0)
        spread = jnp.where(place == dest0, weight_ref[0:1, :], 0.0) + jnp.where(
            place == dest1, weight_ref[1:2, :], 0.0
        )
        high = spread.astype(bf16)
        low = (spread - high.astype(f32)).astype(bf16)
        cot = cot_ref[...]
        to_chunks(dot(high, cot, 1, 0) + dot(low, cot, 1, 0), scratch)
        out_ref[...] = scratch[...].astype(bf16)

    return body


def pick_body(dest_ref, pick_ref):
    tokens, slots = pick_ref.shape
    row = lax.broadcasted_iota(jnp.int32, (tokens, tokens), 0)
    col = lax.broadcasted_iota(jnp.int32, (tokens, tokens), 1)
    dest0, dest1 = (
        jnp.sum(jnp.where(row == col, dest_ref[k : k + 1, :].astype(f32), 0.0), axis=1, keepdims=True)
        .astype(jnp.int32)
        for k in range(2)
    )
    place = lax.broadcasted_iota(jnp.int32, (tokens, slots), 1)
    pick_ref[...] = ((place == dest0) | (place == dest1)).astype(f32).astype(bf16)


def factors_body(rows_ref, gate_ref, up_ref, act_ref, for_up_ref, for_gate_ref):
    block = rows_ref.shape[0] // 3

    def step(i, _):
        at = pl.ds(pl.multiple_of(i * block, block), block)
        rows = rows_ref[at, :]
        gate_lin = dot(rows, gate_ref[...], 1, 0)
        up_lin = dot(rows, up_ref[...], 1, 0)
        gate_c = jnp.minimum(gate_lin, clamp_limit)
        up_c = jnp.clip(up_lin, -clamp_limit, clamp_limit)
        sigma = jax.nn.sigmoid(swish_alpha * gate_c)
        swish = gate_c * sigma
        act_ref[at, :] = ((up_c + 1.0) * swish).astype(bf16)
        up_open = (up_lin > -clamp_limit) & (up_lin < clamp_limit)
        for_up_ref[at, :] = jnp.where(up_open, swish, 0.0).astype(bf16)
        slope = (up_c + 1.0) * (sigma + swish_alpha * swish * (1.0 - sigma))
        for_gate_ref[at, :] = jnp.where(gate_lin < clamp_limit, slope, 0.0).astype(bf16)
        return 0

    lax.fori_loop(0, 3, step, 0)


def partial_act_body(chunks_ref, far_ref, next_ref, prev_ref, own_ref, *outs_scratch):
    rows_ref, far_top, far_bot, next_top, next_bot, prev_top, prev_bot, own_out, scratch = outs_scratch
    n, width = rows_ref.shape
    half = n // 2
    rows = from_chunks(chunks_ref[...], scratch, n, width // LANES)
    rows_ref[...] = rows
    for weight, top, bot in (
        (far_ref, far_top, far_bot),
        (next_ref, next_top, next_bot),
        (prev_ref, prev_top, prev_bot),
    ):
        value = dot(rows, weight[...], 1, 1).astype(bf16)
        top[...] = value[:half]
        bot[...] = value[half:]
    own_out[...] = dot(rows, own_ref[...], 1, 1).astype(bf16)


def block_of(ref, index, size):
    return ref[pl.ds(pl.multiple_of(index * size, size), size), :]


def hidden_grad_body(
    at_ref, own_ref, prev_top, near_top, next_bot, near_bot, up_ref, gate_ref, wg_ref, wu_ref,
    d_gate_ref, d_up_ref, far_top, far_bot,
):
    half = prev_top.shape[0]
    size = far_top.shape[1]
    count = wg_ref.shape[0] // size
    own = own_ref[...].astype(f32)
    top = own[:half] + prev_top[...].astype(f32) + near_top[...].astype(f32)
    bot = own[half:] + next_bot[...].astype(f32) + near_bot[...].astype(f32)
    d_act = jnp.concatenate([top, bot], axis=0)
    d_gate = (d_act * gate_ref[...].astype(f32)).astype(bf16)
    d_up = (d_act * up_ref[...].astype(f32)).astype(bf16)
    d_gate_ref[...] = d_gate
    d_up_ref[...] = d_up
    far = lax.rem(at_ref[0] + 2, count)
    value = dot(d_gate, block_of(wg_ref, far, size), 1, 1) + dot(d_up, block_of(wu_ref, far, size), 1, 1)
    value = value.astype(bf16)
    far_top[...] = value[:half]
    far_bot[...] = value[half:]


def input_grad_body(
    at_ref, d_gate_ref, d_up_ref, wg_ref, wu_ref, next_top, next_bot, prev_top, prev_bot, own_out
):
    half = next_top.shape[0]
    size = own_out.shape[1]
    count = wg_ref.shape[0] // size
    d_gate, d_up = d_gate_ref[...], d_up_ref[...]

    def part(shift):
        at = lax.rem(at_ref[0] + shift, count)
        value = dot(d_gate, block_of(wg_ref, at, size), 1, 1)
        value = value + dot(d_up, block_of(wu_ref, at, size), 1, 1)
        return value.astype(bf16)

    value = part(1)
    next_bot[...] = value[half:]
    next_top[...] = value[:half]
    value = part(count - 1)
    prev_top[...] = value[:half]
    prev_bot[...] = value[half:]
    own_out[...] = part(0)


def total_body(own_ref, prev_top, near_top, next_bot, near_bot, out_ref, scratch):
    half = prev_top.shape[0]
    own = own_ref[...].astype(f32)
    top = own[:half] + prev_top[...].astype(f32) + near_top[...].astype(f32)
    bot = own[half:] + next_bot[...].astype(f32) + near_bot[...].astype(f32)
    to_chunks(jnp.concatenate([top, bot], axis=0), scratch)
    out_ref[...] = scratch[...].astype(bf16)


def combine_body(chunks_ref, pick_ref, cot_ref, mix_ref, scratch):
    slots = pick_ref.shape[1]
    rows = from_chunks(chunks_ref[...], scratch, slots, cot_ref.shape[1] // LANES)
    mix = (cot_ref[...].astype(f32) + dot(pick_ref[...], rows, 1, 0)).astype(bf16)
    mix_ref[...] = mix


def down_near_body(at_ref, act_ref, *refs):
    *rows, out_ref = refs
    size = rows[0].shape[1]
    count = out_ref.shape[1] // size
    act = act_ref[...]
    for rows_ref, shift in zip(rows, (0, 1, count - 1)):
        at = lax.rem(at_ref[0] + shift, count)
        value = dot(act, rows_ref[...], 0, 0)
        out_ref[:, pl.ds(pl.multiple_of(at * size, size), size)] = value.astype(bf16)


def down_far_body(at_ref, act_ref, rows_ref, near_ref, out_ref, block, sem):
    size = rows_ref.shape[1]
    block[...] = dot(act_ref[...], rows_ref[...], 0, 0).astype(bf16)
    at = lax.rem(at_ref[0] + 2, out_ref.shape[1] // size)
    put = pltpu.make_async_copy(
        block, out_ref.at[:, pl.ds(pl.multiple_of(at * size, size), size)], sem
    )
    put.start()
    put.wait()


def proj_grad_body(columns):
    def body(core_ref, act_ref, *refs):
        *mixes, send_ref, keep_ref = refs
        size = mixes[0].shape[1]
        rows = act_ref.shape[1] // 2
        block = rows // columns
        first = core_ref[0] == 0
        act = act_ref[...]
        for s, mix_ref in enumerate(mixes):
            value = dot(act, mix_ref[...], 0, 0).reshape(block // 8, columns, 2, 8, size)
            for x in range(columns):
                zero, one = (value[:, x, core].reshape(block, size) for core in range(2))
                at = (slice(x * block, (x + 1) * block), slice(s * size, (s + 1) * size))
                send_ref[at] = jnp.where(first, one, zero).astype(bf16)
                keep_ref[at] = jnp.where(first, zero, one).astype(bf16)

    return body


def pair_sum_body(at_ref, near_ref, near_in_ref, far_ref, far_in_ref, *outs):
    size = outs[0].shape[0]
    count = near_ref.shape[0] // size
    near = near_ref.shape[1]
    for out_ref, shift in zip(outs, (0, 1, count - 1, 2)):
        at = lax.rem(at_ref[0] + shift, count)

        def total(one_ref, two_ref):
            one, two = block_of(one_ref, at, size), block_of(two_ref, at, size)
            return (one.astype(f32) + two.astype(f32)).astype(bf16)

        out_ref[:, :near] = total(near_ref, near_in_ref)
        out_ref[:, near:] = total(far_ref, far_in_ref)


def four_sum_body(*refs):
    *terms, out_ref = refs
    out_ref[...] = sum(term[...].astype(f32) for term in terms).astype(bf16)


def proj_total_body(at_ref, terms_ref, out_ref):
    rows, width = out_ref.shape
    count = 4
    terms = terms_ref[...].astype(f32)
    total = jnp.sum(terms.reshape(terms.shape[0] // rows, rows, width), axis=0)
    size = width // count
    for s, shift in enumerate((0, 1, count - 1, 2)):
        at = lax.rem(at_ref[0] + shift, count)
        out_ref[:, pl.ds(pl.multiple_of(at * size, size), size)] = total[:, s * size : (s + 1) * size]


def split(value, pieces):
    terms = []
    for _ in range(pieces):
        terms.append(value.astype(bf16))
        value = value - terms[-1].astype(f32)
    return terms


def row_sums(first, second, out_ref):
    ones = jnp.ones((8, first.shape[1]), bf16)
    one = sum(dot(ones, term, 1, 1) for term in split(first, 3))
    two = sum(dot(ones, term, 1, 1) for term in split(second, 3))
    row = lax.broadcasted_iota(jnp.int32, out_ref.shape, 0)
    out_ref[...] = jnp.where(row == 0, one, jnp.where(row == 1, two, 0.0))


def along_rows(sums, index):
    row = lax.broadcasted_iota(jnp.int32, (8, LANES), 0)
    chosen = (row == index).astype(f32).astype(bf16)
    return sum(dot(term, chosen, 0, 0) for term in split(sums, 3))


def widened(value, lanes):
    return jnp.concatenate([value] * (lanes // LANES), axis=1)


def stats_body(conv_ref, out_ref):
    conv = conv_ref[...].astype(f32)
    row_sums(conv, conv * conv, out_ref)


def norm_body(channels):
    def body(own, one, two, three, conv_ref, gain_ref, *outs):
        sums = own[...] + one[...] + two[...] + three[...]
        width = conv_ref.shape[1]
        mean = along_rows(sums, 0) / channels
        var = along_rows(sums, 1) / channels - mean * mean
        rstd = lax.rsqrt(var + norm_epsilon)
        xhat = (conv_ref[...].astype(f32) - widened(mean, width)) * widened(rstd, width)
        gain = gain_ref[...]
        normed = xhat * gain
        sigma = jax.nn.sigmoid(normed)
        act_ref, xhat_ref, slope_ref, rstd_ref = outs
        act_ref[...] = (normed * sigma).astype(bf16)
        rstd_ref[...] = rstd
        xhat_ref[...] = xhat
        slope_ref[...] = sigma * (1.0 + normed * (1.0 - sigma)) * gain

    return body


def norm_grad_body(at_ref, own, following, previous, far, proj_ref, xhat_ref, slope_ref, dxh_ref, sums_ref):
    size = own.shape[1]
    count = proj_ref.shape[1] // size
    value = None
    for shift, mix_ref in ((0, own), (1, following), (count - 1, previous), (2, far)):
        at = lax.rem(at_ref[0] + shift, count)
        weight = proj_ref[:, pl.ds(pl.multiple_of(at * size, size), size)]
        term = dot(mix_ref[...], weight, 1, 1)
        value = term if value is None else value + term
    dxh = value * slope_ref[...]
    dxh_ref[...] = dxh
    row_sums(dxh, dxh * xhat_ref[...], sums_ref)


def conv_grad_body(channels):
    def body(own, one, two, three, dxh_ref, xhat_ref, rstd_ref, out_ref, edge_ref):
        sums = own[...] + one[...] + two[...] + three[...]
        width = dxh_ref.shape[1]
        first = widened(along_rows(sums, 0) / channels, width)
        second = widened(along_rows(sums, 1) / channels, width)
        value = widened(rstd_ref[...], width) * (dxh_ref[...] - first - xhat_ref[...] * second)
        out_ref[...] = value
        edge_ref[...] = value[: edge_ref.shape[0]]

    return body


def conv_body(grad_ref, edge_ref, taps_ref, value_ref, gate_ref, value_out, gate_out, extended, moved):
    tokens, width = grad_ref.shape
    reach = taps_ref.shape[0]
    extended[:tokens, :] = grad_ref[...]
    extended[tokens:, :] = edge_ref[...]
    rows = moved.shape[1]
    block = 64

    def step(i, _):
        lanes = pl.ds(pl.multiple_of(i * LANES, LANES), LANES)
        for r in range(8):
            moved[r] = extended[r : r + rows, lanes]
        for start in range(0, tokens, block):
            total = jnp.zeros((block, LANES), f32)
            for offset in range(reach):
                tap = taps_ref[reach - 1 - offset : reach - offset, lanes]
                begin = start + offset // 8 * 8
                total = total + tap * moved[offset % 8, begin : begin + block, :]
            at = slice(start, start + block)
            sigma = jax.nn.sigmoid(gate_ref[at, lanes].astype(f32))
            scaled = total * sigma
            value_out[at, lanes] = scaled.astype(bf16)
            gate = scaled * value_ref[at, lanes].astype(f32) * (1.0 - sigma)
            gate_out[at, lanes] = gate.astype(bf16)
        return 0

    lax.fori_loop(0, width // LANES, step, 0)


def weight_grad_body(rows_ref, gate_ref, up_ref, gate_out, up_out):
    size = gate_ref.shape[1]
    both = jnp.concatenate([gate_ref[...], up_ref[...]], axis=1)

    def step(i, _):
        at = pl.ds(pl.multiple_of(i * size, size), size)
        value = dot(rows_ref[:, at], both, 0, 0)
        gate_out[at, :] = value[:, :size].astype(bf16)
        up_out[at, :] = value[:, size:].astype(bf16)
        return 0

    lax.fori_loop(0, rows_ref.shape[1] // size, step, 0)


def near_body(one_ref, two_ref, out_ref):
    out_ref[...] = (one_ref[...].astype(f32) + two_ref[...].astype(f32)).astype(bf16)


def near_sum(one, two):
    (value,) = kernel(near_body, (struct(one.shape),), one, two, flops=one.size, limit=4)
    return value


def exchanged(value):
    return shifted(value, TP, 1), shifted(value, TP, -1), shifted(value, TP, 2)


def reduce_over_ring(far_top, far_bot, rest):
    far_top_in = shifted(far_top, TP, 1)
    far_bot_in = shifted(far_bot, TP, -1)
    next_top, next_bot, prev_top, prev_bot, own = rest
    next_bot_in = shifted(next_bot, TP, 1)
    prev_top_in = shifted(prev_top, TP, -1)
    near_top = near_sum(next_top, far_top_in)
    near_bot = near_sum(prev_bot, far_bot_in)
    near_top_in = shifted(near_top, TP, 1)
    near_bot_in = shifted(near_bot, TP, -1)
    return own, prev_top_in, near_top_in, next_bot_in, near_bot_in


def per_device(
    cot_out,
    route_ids,
    route_weight,
    expert_inputs,
    w_gate,
    w_up,
    w_down,
    w_proj,
    conv_out,
    channel_norm_gain,
    taps,
    value_pre,
    gate_pre,
):
    experts = lax.axis_size(SP)
    ways = lax.axis_size(TP)
    tok_rows = cot_out.shape[0]
    slot_rows = expert_inputs.shape[1]
    capacity = slot_rows // experts
    local_cols = cot_out.shape[1]
    hidden = w_down.shape[1]
    half = slot_rows // 2
    parts = local_cols // LANES
    chunk_rows = slot_rows * parts
    at = lax.axis_index(TP)
    at_ref = at.reshape(1).astype(jnp.int32)
    core_ref = lax.axis_index(CORE).reshape(1).astype(jnp.int32)
    rows_in, gate_weight, up_weight, down_weight = expert_inputs[0], w_gate[0], w_up[0], w_down[0]
    chunk_scratch = pltpu.VMEM((chunk_rows, LANES), f32)

    outgoing, dest = kernel(
        dispatch_body(experts, capacity),
        (struct((chunk_rows, LANES)), struct((2, tok_rows), jnp.int32)),
        route_ids.T, route_weight.T, cot_out,
        flops=4 * tok_rows * slot_rows * local_cols, scratch=(chunk_scratch,),
        staged=(), to_hbm=(0, 1),
    )
    moved = lax.all_to_all(
        outgoing.reshape(experts, chunk_rows // experts, LANES), SP, 0, 0, tiled=True
    )
    dest, conv_late, down_late, rows_late, gate_late, up_late = lax.optimization_barrier(
        (dest, conv_out, down_weight, rows_in, gate_weight, up_weight)
    )

    def down_block(shift):
        start = (at + shift) % ways * local_cols
        return lax.dynamic_slice_in_dim(down_late, start, local_cols, 1)

    down_own = down_block(0)
    down_next = shifted(down_block(ways - 1), TP, -1)
    down_prev = shifted(down_block(1), TP, 1)
    down_far = shifted(down_block(2), TP, 2)
    act, for_up, for_gate = kernel(
        factors_body,
        (struct((slot_rows, hidden)),) * 3,
        rows_late, gate_late, up_late,
        flops=4 * slot_rows * hidden * local_cols * ways,
    )
    (pick,) = kernel(
        pick_body, (struct((tok_rows, slot_rows)),), dest, flops=tok_rows * slot_rows * 8
    )
    channel_total = local_cols * ways
    tokens_8 = struct((8, tok_rows), f32)
    block = struct((tok_rows, local_cols), f32)
    (stats,) = kernel(stats_body, (tokens_8,), conv_late, flops=48 * tok_rows * local_cols, limit=8)
    stats_in = exchanged(stats)
    gain = channel_norm_gain.reshape(1, local_cols)
    moved, act, for_up, for_gate, pick, stats_in = lax.optimization_barrier(
        (moved, act, for_up, for_gate, pick, stats_in)
    )

    rows_cot, far_top, far_bot, *rest = kernel(
        partial_act_body,
        (struct((slot_rows, local_cols)),) + (struct((half, hidden)),) * 6
        + (struct((slot_rows, hidden)),),
        moved.reshape(chunk_rows, LANES), down_far, down_next, down_prev, down_own,
        flops=2 * slot_rows * local_cols * hidden * ways,
        scratch=(chunk_scratch,), to_hbm=(0,),
    )
    act_terms = reduce_over_ring(far_top, far_bot, rest)
    d_gate, d_up, far_top, far_bot = kernel(
        hidden_grad_body,
        (struct((slot_rows, hidden)),) * 2 + (struct((half, local_cols)),) * 2,
        at_ref, *act_terms, for_up, for_gate, gate_weight, up_weight,
        flops=4 * slot_rows * local_cols * hidden, smem=1,
    )
    rest = kernel(
        input_grad_body,
        (struct((half, local_cols)),) * 4 + (struct((slot_rows, local_cols)),),
        at_ref, d_gate, d_up, gate_weight, up_weight,
        flops=12 * slot_rows * local_cols * hidden, smem=1,
    )
    grad_terms = reduce_over_ring(far_top, far_bot, rest)
    (returning,) = kernel(
        total_body,
        (struct((chunk_rows, LANES)),),
        *grad_terms,
        flops=slot_rows * local_cols * 8, scratch=(chunk_scratch,),
    )
    coming = lax.all_to_all(
        returning.reshape(experts, chunk_rows // experts, LANES), SP, 0, 0, tiled=True
    )
    grad_gate_part, grad_up_part = kernel(
        weight_grad_body,
        (struct((local_cols * ways, hidden)),) * 2,
        rows_in, d_gate, d_up,
        flops=4 * slot_rows * hidden * local_cols * ways, to_hbm=(0, 1),
    )
    rows_cot, _ = lax.optimization_barrier((rows_cot, returning))
    rows_prev = shifted(rows_cot, TP, 1)
    rows_next = shifted(rows_cot, TP, -1)
    coming, grad_gate_part, grad_up_part = lax.optimization_barrier(
        (coming, grad_gate_part, grad_up_part)
    )
    (mix,) = kernel(
        combine_body,
        (struct((tok_rows, local_cols)),),
        coming.reshape(chunk_rows, LANES), pick, cot_out,
        flops=2 * tok_rows * slot_rows * local_cols, scratch=(chunk_scratch,),
    )
    mix_far = shifted(mix, TP, 2)
    mix_prev = shifted(mix, TP, 1)
    mix_next = shifted(mix, TP, -1)
    conv_mid, _ = lax.optimization_barrier((conv_out, mix))
    act_conv, xhat, slope, rstd = kernel(
        norm_body(channel_total),
        (struct((tok_rows, local_cols)), block, block, struct((tok_rows, LANES), f32)),
        stats, *stats_in, conv_mid, gain,
        flops=20 * tok_rows * local_cols, limit=8, staged=(),
    )
    columns, planes = lax.axis_size(COLUMN), lax.axis_size(PLANE)
    width = local_cols * ways
    core_rows = local_cols // 2
    column_rows = core_rows // columns

    def proj_terms(mixes):
        return kernel(
            proj_grad_body(columns),
            (struct((core_rows, local_cols * len(mixes))),) * 2,
            core_ref, act_conv, *mixes,
            flops=2 * len(mixes) * tok_rows * local_cols * local_cols, smem=1,
            to_hbm=(1,),
        )

    send, keep = proj_terms((mix, mix_next, mix_prev))
    came = shifted(send, CORE, 1)
    send_far, keep_far = proj_terms((mix_far,))
    came_far = shifted(send_far, CORE, 1)
    pair_own, pair_next, pair_prev, pair_far = kernel(
        pair_sum_body,
        (struct((column_rows, width)),) * 4,
        lax.axis_index(COLUMN).reshape(1).astype(jnp.int32), keep, came, keep_far, came_far,
        flops=core_rows * width, smem=1, limit=8, staged=(1, 3),
    )
    far_pair = shifted(pair_far, COLUMN, 2)
    near_pairs = (shifted(pair_next, COLUMN, 1), shifted(pair_prev, COLUMN, -1))
    (column_sum,) = kernel(
        four_sum_body,
        (struct((column_rows, width)),),
        pair_own, far_pair, *near_pairs,
        flops=column_rows * width * 4, limit=8,
    )
    terms = lax.all_to_all(
        column_sum.reshape(planes, column_rows // planes, width), PLANE, 0, 0, tiled=True
    )
    (grad_proj,) = kernel(
        proj_total_body,
        (struct((column_rows // planes, width), f32),),
        at_ref, terms.reshape(column_rows, width),
        flops=column_rows * width, smem=1, limit=8, to_hbm=(0,),
    )
    dxh, sums = kernel(
        norm_grad_body,
        (block, tokens_8),
        at_ref, mix, mix_next, mix_prev, mix_far, w_proj, xhat, slope,
        flops=2 * tok_rows * local_cols * local_cols * ways, smem=1,
        staged=(0, 1, 2, 3, 5, 6),
    )
    sums_in = exchanged(sums)
    rows_far = shifted(rows_cot, TP, 2)
    (grad_down,) = kernel(
        down_near_body,
        (struct((hidden, width)),),
        at_ref, act, rows_cot, rows_next, rows_prev,
        flops=6 * slot_rows * hidden * local_cols, smem=1, to_hbm=(0,), staged=(),
    )
    hbm = pl.BlockSpec(memory_space=pltpu.HBM)
    vmem = pl.BlockSpec(memory_space=pltpu.VMEM)
    grad_down = pl.pallas_call(
        down_far_body,
        out_shape=struct((hidden, width)),
        in_specs=[pl.BlockSpec(memory_space=pltpu.SMEM), vmem, vmem, hbm],
        out_specs=hbm,
        scratch_shapes=[pltpu.VMEM((hidden, local_cols), bf16), pltpu.SemaphoreType.DMA],
        input_output_aliases={3: 0},
        cost_estimate=pl.CostEstimate(
            flops=2 * slot_rows * hidden * local_cols, transcendentals=0, bytes_accessed=1 << 20
        ),
        compiler_params=pltpu.CompilerParams(vmem_limit_bytes=24 << 20),
        name="down_far",
    )(
        at_ref,
        *(pltpu.with_memory_space_constraint(v, pltpu.HBM) for v in (act, rows_far, grad_down)),
    )
    reach = taps.shape[0]
    convolution_gradient, edge = kernel(
        conv_grad_body(channel_total),
        (block, struct((32, local_cols), f32)),
        sums, *sums_in, dxh, xhat, rstd,
        flops=8 * tok_rows * local_cols, limit=8,
    )
    following = passed_along(edge, SP, -1)
    following, grad_down = lax.optimization_barrier((following, grad_down))
    grad_value, grad_gate = kernel(
        conv_body,
        (struct((tok_rows, local_cols)),) * 2,
        convolution_gradient, following, taps, value_pre, gate_pre,
        flops=2 * reach * tok_rows * local_cols, limit=8, to_hbm=(0, 1),
        staged=(0, 1),
        scratch=(
            pltpu.VMEM((tok_rows + edge.shape[0], local_cols), f32),
            pltpu.VMEM((8, tok_rows + 24, LANES), f32),
        ),
    )
    return (
        grad_gate_part[None],
        grad_up_part[None],
        grad_down[None],
        grad_proj,
        grad_value,
        grad_gate,
    )


def solution(mesh):
    finer = Mesh(mesh.devices.reshape(8, 4, 2, mesh.shape["tp"]), ("sp_0", "sp_1", "sp_2", "tp"))
    placed = (
        P(SP, "tp"),
        P(SP, None),
        P(SP, None),
        P(SP, None, None),
        P(SP, None, "tp"),
        P(SP, None, "tp"),
        P(SP, "tp", None),
        P("tp", None),
        P(SP, "tp"),
        P("tp"),
        P(None, "tp"),
        P(SP, "tp"),
        P(SP, "tp"),
    )

    return jax.shard_map(
        per_device,
        mesh=finer,
        in_specs=placed,
        out_specs=(
            P(SP, None, "tp"),
            P(SP, None, "tp"),
            P(SP, "tp", None),
            P(TP_SP, None),
            P(SP, "tp"),
            P(SP, "tp"),
        ),
        check_vma=False,
    )
```
